128 devices in a mesh: sp: 16 (over z, x), tp: 8 (over y, core).
Axes of the slice: x: 4, y: 4, z: 4, core: 2. Of those that a mesh axis runs over, the one named last changes fastest.
Arguments:
- a_lin: bfloat16 [16384, 1024], P('sp', 'tp'), may hold values from -6 to 6
- a_gate: bfloat16 [16384, 1024], P('sp', 'tp'), may hold values from -9 to 9
- conv_weight: bfloat16 [31, 1024], P(None, 'tp'), may hold values from -7 to 7
- ln_gain: bfloat16 [1024], P('tp'), may hold values from 0.099609375 to 1.8984375
- ln_bias: bfloat16 [1024], P('tp'), may hold values from -3 to 3
- proj_weight: bfloat16 [1024, 2048], replicated, may hold values from -0.1875 to 0.1875
- residual: bfloat16 [16384, 2048], P(('sp', 'tp')), may hold values from -6 to 6
- mix_gain: bfloat16 [2048], replicated, may hold values from 0.099609375 to 1.8984375
- ffn_gain: bfloat16 [2048], replicated, may hold values from 0.099609375 to 1.8984375
- routes: int32 [16384, 2], P(('sp', 'tp')), may hold values from 0 to 15, all different within a row; in each aligned block of 128 rows (0 to 127, 128 to 255, ...) at most 20 rows name the same one
- route_weights: float32 [16384, 2], P(('sp', 'tp')), may hold values from 0.1 to 1
- gate_weight: bfloat16 [16, 2048, 7168], P('sp', None, 'tp'), may hold values from -0.125 to 0.125
- up_weight: bfloat16 [16, 2048, 7168], P('sp', None, 'tp'), may hold values from -0.125 to 0.125
- down_weight: bfloat16 [16, 7168, 2048], P('sp', 'tp'), may hold values from -0.0625 to 0.0625
- out_gain: bfloat16 [2048], replicated, may hold values from 0.099609375 to 1.8984375
Outputs:
- layer_out: bfloat16 [16384, 2048], P(('sp', 'tp'))
The draws below stay inside these ranges and needn't reach their ends.
Inputs may be any that keep to these rules, and one draw needn't show every extreme that they name: In the rows of one device (128 aligned rows) no expert is named by more than 20 routes, a bound that some block reaches; the entries of one row differ.
All inputs are finite; a program needn't handle non-finite values.
Results may differ from the reference program's by a relative error of at most 0.018.
Values may be sent and summed in bfloat16 or wider, within the bound.
A program may use at most 128 MiB of HBM per device.

```python
import math
import jax
import jax.numpy as jnp
import numpy as np
from jax import lax

D = 2048
D_A = 1024
FF = 7168
CONV = 31
TOPK = 2
TOK_DEV = 128
TOKENS = 16384
EXPERTS = 16
CAP = 20
N_SP = 16
N_TP = 8


def draw_conv_weight(key, part):
    first_key, second_key = jax.random.split(jax.random.fold_in(key, 17))
    filter_taps = jax.random.uniform(first_key, (CONV, D_A), jnp.float32, -1.0, 1.0)
    roughness = jnp.exp(jax.random.uniform(second_key, (D_A,), jnp.float32, -0.7, 0.7))
    position = jnp.arange(D_A, dtype=jnp.float32) / D_A
    rising = 3.0 ** position
    values = filter_taps * (3.0 / CONV) ** 0.5 * roughness[None, :] * rising[None, :]
    return values.astype(jnp.bfloat16)


def levels(key, dims, pieces, low, top_value):
    def one(dim, blocks):
        draws = jax.random.uniform(jax.random.fold_in(jax.random.fold_in(key, 6), dim), (blocks,), jnp.float32, low / len(pieces), top_value / len(pieces))
        return jnp.repeat(jnp.exp(draws), dims[dim] // blocks).reshape((-1,) + (1,) * (len(dims) - dim - 1))

    loudness = one(*pieces[0])
    for cut in pieces[1:]:
        loudness = loudness * one(*cut)
    return loudness


def routed_block(rng, own, number, rows, count, top, reach, skew):
    order = jax.random.permutation(rng, count)
    crowded, usual = shares(count, rows * top, reach, skew, True), shares(count, rows * top, reach, skew, False)
    places = jnp.arange(count)

    def named(lengths, offset_by):
        used = int((lengths > 0).sum())
        fixed = max(1, used // 4)
        passed = fixed + (places - fixed + offset_by * (used - fixed)) % max(1, count - fixed)
        return jnp.zeros((count,), jnp.int32).at[order[jnp.where(places < fixed, places, passed)]].set(jnp.asarray(lengths, jnp.int32))

    lengths = jnp.where(number % 4 == 0, named(crowded, number // 4), named(usual, number - number // 4 - 1))
    mixed = jax.random.permutation(jax.random.fold_in(own, 3), count)
    donor, sink = mixed[0:count // 2 * 2:2], mixed[1:count // 2 * 2:2]
    margin = jnp.minimum(lengths[donor] - 1, reach - lengths[sink]) // 2
    margin = jnp.where((donor == order[0]) | (sink == order[0]) | (lengths[sink] == 0), 0, jnp.maximum(margin, 0))
    passed = jax.random.randint(jax.random.fold_in(own, 4), (count // 2,), 0, 1 << 20) % (margin + 1)
    lengths = lengths.at[donor].add(-passed).at[sink].add(passed)
    items = jnp.searchsorted(jnp.cumsum(lengths), jnp.arange(rows * top), side="right").astype(jnp.int32)
    listing = items.reshape(top, rows).T
    listing = listing[jax.random.permutation(jax.random.fold_in(own, 1), rows)]
    offset_by = jax.random.randint(jax.random.fold_in(own, 2), (rows, 1), 0, top)
    return jnp.take_along_axis(listing, (jnp.arange(top)[None, :] + offset_by) % top, axis=1)


def shares(number_of, total, limit, skew, full):
    loads = [(1 << 20) // math.isqrt(grade ** skew) + 1 for grade in range(1, number_of + 1)]
    largest = limit if full else min(limit, max(-(-total // number_of), total * loads[0] // sum(loads)))
    least = 1 if total - largest >= number_of - 1 else 0
    counts, rest = [largest] + [least] * (number_of - 1), total - largest - least * (number_of - 1)
    while rest > 0:
        movable = [i for i in range(1, number_of) if counts[i] < largest] or [i for i in range(1, number_of) if counts[i] < limit]
        whole, remaining = sum([loads[i] for i in movable]), rest
        for i in movable:
            addition = min(limit - counts[i], max(1, remaining * loads[i] // whole), rest)
            counts[i] = counts[i] + addition
            rest = rest - addition
    return np.array(counts)


def normal_values(key, extent, deviation, bound, shards=(), kind=jnp.bfloat16):
    values = deviation * jax.random.normal(key, extent, jnp.float32)
    if shards:
        values = values * levels(key, extent, shards, -0.22, 0.18)
    return jnp.clip(values, -bound, bound).astype(kind)


def setup_inputs(seed: int = 0) -> dict:
    splits = jax.random.split(jax.random.key(seed), 16)
    a_lin = normal_values(splits[0], (TOKENS, D_A), 1.0, 6.0, ((0, 16), (1, 8)))
    a_gate = normal_values(splits[1], (TOKENS, D_A), 1.5, 9.0, ((0, 16), (1, 8)))
    conv_weight = draw_conv_weight(jax.random.fold_in(splits[15], 71), 0)
    ln_gain = jnp.clip(1.0 + 0.18 * jax.random.normal(splits[3], (D_A,), jnp.float32), 0.099609375, 1.8984375).astype(jnp.bfloat16)
    ln_bias = normal_values(splits[4], (D_A,), 0.5, 3.0, ((0, 8),))
    proj_weight = normal_values(splits[5], (D_A, D), D_A ** -0.5, 0.1875)
    residual = normal_values(splits[6], (TOKENS, D), 1.0, 6.0, ((0, 128),))
    mix_gain = jnp.clip(1.0 + 0.18 * jax.random.normal(splits[7], (D,), jnp.float32), 0.099609375, 1.8984375).astype(jnp.bfloat16)
    ffn_gain = jnp.clip(1.0 + 0.18 * jax.random.normal(splits[8], (D,), jnp.float32), 0.099609375, 1.8984375).astype(jnp.bfloat16)
    routes_keys = jax.random.split(jax.random.fold_in(splits[9], 1), TOKENS // TOK_DEV)
    routes_turns = jax.random.permutation(jax.random.fold_in(splits[9], 3), TOKENS // TOK_DEV)
    routes = jax.vmap(lambda own, number: routed_block(jax.random.fold_in(splits[9], 2), own, number, TOK_DEV, EXPERTS, TOPK, CAP, 2))(routes_keys, routes_turns).reshape((TOKENS, TOPK))
    route_weights = jnp.clip(0.1 + 0.9 * jax.random.uniform(splits[10], (TOKENS, TOPK), jnp.float32) ** levels(splits[10], (TOKENS, TOPK), ((0, 128),), -0.2, 0.2), 0.1, 1.0)
    gate_weight = normal_values(splits[11], (EXPERTS, D, FF), D ** -0.5, 0.125, ((0, 16), (2, 8)))
    up_weight = normal_values(splits[12], (EXPERTS, D, FF), D ** -0.5, 0.125, ((0, 16), (2, 8)))
    down_weight = normal_values(splits[13], (EXPERTS, FF, D), FF ** -0.5, 0.0625, ((0, 16), (1, 8)))
    out_gain = jnp.clip(1.0 + 0.18 * jax.random.normal(splits[14], (D,), jnp.float32), 0.099609375, 1.8984375).astype(jnp.bfloat16)
    return dict(a_lin=a_lin, a_gate=a_gate, conv_weight=conv_weight, ln_gain=ln_gain, ln_bias=ln_bias, proj_weight=proj_weight, residual=residual, mix_gain=mix_gain, ffn_gain=ffn_gain, routes=routes, route_weights=route_weights, gate_weight=gate_weight, up_weight=up_weight, down_weight=down_weight, out_gain=out_gain)


def reference(a_lin, a_gate, conv_weight, ln_gain, ln_bias, proj_weight, residual, mix_gain, ffn_gain, routes, route_weights, gate_weight, up_weight, down_weight, out_gain):
    gated = (a_lin.astype(jnp.float32) * jax.nn.sigmoid(a_gate.astype(jnp.float32))).astype(jnp.bfloat16)
    padded = jnp.concatenate([jnp.zeros((CONV - 1, D_A), jnp.bfloat16), gated], 0).astype(jnp.float32)
    filter_taps = conv_weight.astype(jnp.float32)
    conv_out = filter_taps[0] * padded[0:TOKENS]
    for offset in range(1, CONV):
        conv_out = conv_out + filter_taps[offset] * padded[offset:offset + TOKENS]
    row_total = lax.optimization_barrier(jnp.sum(conv_out, axis=1))
    squares = lax.optimization_barrier(jnp.sum(conv_out * conv_out, axis=1))
    row_mean = row_total / D_A
    row_var = squares / D_A - row_mean * row_mean
    scaled = (conv_out - row_mean[:, None]) * lax.rsqrt(row_var[:, None] + 1e-05)
    scaled = scaled * ln_gain.astype(jnp.float32) + ln_bias.astype(jnp.float32)
    activated = jax.nn.silu(scaled).astype(jnp.bfloat16)
    branch = jnp.dot(activated, proj_weight, preferred_element_type=jnp.float32).astype(jnp.bfloat16)
    branch_f = lax.optimization_barrier(branch).astype(jnp.float32)
    branch_scale = lax.rsqrt(lax.optimization_barrier(jnp.mean(branch_f * branch_f, axis=1, keepdims=True)) + 1e-06)
    stream = residual.astype(jnp.float32) + branch_f * branch_scale * mix_gain.astype(jnp.float32)
    stream_scale = lax.rsqrt(lax.optimization_barrier(jnp.mean(stream * stream, axis=1, keepdims=True)) + 1e-06)
    normed = (stream * stream_scale * ffn_gain.astype(jnp.float32)).astype(jnp.bfloat16)
    blocks = N_SP * N_TP
    flat_routes = routes.reshape(blocks, TOK_DEV * TOPK)
    matches = (flat_routes[:, :, None] == jnp.arange(EXPERTS, dtype=jnp.int32)[None, None, :]).astype(jnp.int32)
    before = jnp.cumsum(matches, axis=1) - matches
    slot_index = lax.optimization_barrier(jnp.sum(before * matches, axis=2))
    block_ids = jnp.arange(blocks, dtype=jnp.int32)[:, None]
    target = ((flat_routes * blocks + block_ids) * CAP + slot_index).reshape(-1).astype(jnp.int32)
    source_rows = jnp.repeat(normed, TOPK, axis=0)
    buffer = jnp.zeros((EXPERTS * blocks * CAP, D), jnp.bfloat16).at[target].set(source_rows)
    buffer = buffer.reshape(EXPERTS, blocks * CAP, D)
    width_block = FF // N_TP

    def one_expert(inputs):
        rows_in, w_gate, w_up, w_down = inputs
        accum = jnp.zeros((rows_in.shape[0], D), jnp.float32)
        for part_index in range(N_TP):
            low = part_index * width_block
            gate_proj = jnp.dot(rows_in, w_gate[:, low:low + width_block], preferred_element_type=jnp.float32)
            up_proj = jnp.dot(rows_in, w_up[:, low:low + width_block], preferred_element_type=jnp.float32)
            hidden = (jax.nn.silu(gate_proj) * up_proj).astype(jnp.bfloat16)
            partial_out = jnp.dot(hidden, w_down[low:low + width_block], preferred_element_type=jnp.float32).astype(jnp.bfloat16)
            accum = accum + lax.optimization_barrier(partial_out).astype(jnp.float32)
        return accum.astype(jnp.bfloat16)
    results = lax.map(one_expert, (buffer, gate_weight, up_weight, down_weight))
    results = lax.optimization_barrier(results).reshape(EXPERTS * blocks * CAP, D)
    picked = results[target].astype(jnp.float32).reshape(TOKENS, TOPK, D)
    expert_mix = lax.optimization_barrier(jnp.sum(picked * route_weights[:, :, None], axis=1))
    mix_scale = lax.rsqrt(lax.optimization_barrier(jnp.mean(expert_mix * expert_mix, axis=1, keepdims=True)) + 1e-06)
    return (stream + expert_mix * mix_scale * out_gain.astype(jnp.float32)).astype(jnp.bfloat16)
```

```python
import functools

import jax
import jax.numpy as jnp
from jax import lax
from jax.experimental import pallas as pl
from jax.experimental.pallas import tpu as pltpu
from jax.sharding import PartitionSpec as P

D = 2048
D_A = 1024
HALF = D // 2
FFB = 896
CAP = 20
PAD = 24
TOK = 128
NG = 4
ROWS = 4 * CAP
PADROWS = 4 * PAD
MESH = pl.DeviceIdType.MESH
BF16 = jnp.bfloat16
F32 = jnp.float32

GROUPS = (
    ((0, 1), (0, 3), (1, 0), (3, 0)),
    ((0, 0), (0, 2), (2, 0), (2, 2)),
    ((2, 1), (2, 3), (1, 2), (3, 2)),
    ((1, 1), (1, 3), (3, 1), (3, 3)),
)
OFFS = tuple(o for g in GROUPS for o in g)
SELF = OFFS.index((0, 0))


def moe_kernel(
    normed_ref,
    stream_ref,
    disp_ref,
    comb_ref,
    gain_ref,
    wg_hbm,
    wu_hbm,
    wd_hbm,
    out_ref,
    wgu,
    wd,
    outg,
    arecv,
    xbuf,
    hbuf,
    pbuf,
    precv,
    r1,
    r2,
    ret_s,
    ret_r,
    wsem,
    a_s,
    a_r,
    g_s,
    g_r,
    s_s,
    s_r,
    t_s,
    t_r,
):
    sp = lax.axis_index("sp")
    tp = lax.axis_index("tp")
    z, x = lax.div(sp, 4), lax.rem(sp, 4)
    y, c = lax.div(tp, 2), lax.rem(tp, 2)

    def sp_at(dz, dx):
        return lax.rem(z + dz, 4) * 4 + lax.rem(x + dx, 4)

    up = lax.rem(y + 1, 4) * 2 + c
    down = lax.rem(y + 3, 4) * 2 + c
    mate = y * 2 + 1 - c

    wcopies = []
    for j in range(7):
        cols = pl.ds(128 * j, 128)
        for h, w in enumerate((wg_hbm, wu_hbm)):
            wcopies.append(
                pltpu.make_async_copy(
                    w.at[0, :, cols], wgu.at[j, :, pl.ds(128 * h, 128)], wsem.at[2 * j + h]
                )
            )
    wcopies.append(pltpu.make_async_copy(wd_hbm.at[0], wd, wsem.at[14]))
    for cp in wcopies:
        cp.start()

    barrier = pltpu.get_barrier_semaphore()
    for o in OFFS:
        if o != (0, 0):
            pl.semaphore_signal(
                barrier, inc=1, device_id={"sp": sp_at(*o), "tp": tp}, device_id_type=MESH
            )
    for t in (up, down, mate):
        pl.semaphore_signal(barrier, inc=1, device_id={"sp": sp, "tp": t}, device_id_type=MESH)
    pl.semaphore_wait(barrier, 18)

    def remote(src, dst, ssem, rsem, spi, tpi):
        return pltpu.make_async_remote_copy(
            src_ref=src,
            dst_ref=dst,
            send_sem=ssem,
            recv_sem=rsem,
            device_id={"sp": spi, "tp": tpi},
            device_id_type=MESH,
        )

    sends = []

    acopies = {}
    for i in range(NG):
        rows = jnp.dot(
            disp_ref[PADROWS * i : PADROWS * (i + 1), :],
            normed_ref[...],
            preferred_element_type=F32,
        )
        outg[4 * i : 4 * i + 4] = rows.astype(BF16).reshape(4, PAD, D)
        for j in range(4 * i, 4 * i + 4):
            if j != SELF:
                acopies[j] = remote(
                    outg.at[j], arecv.at[j], a_s.at[j], a_r.at[j], sp_at(*OFFS[j]), tp
                )
                acopies[j].start()
                sends.append(acopies[j])

    r_i = lax.broadcasted_iota(jnp.int32, (ROWS, PADROWS), 0)
    c_i = lax.broadcasted_iota(jnp.int32, (ROWS, PADROWS), 1)
    q_i = sum((r_i >= CAP * k).astype(jnp.int32) for k in (1, 2, 3))
    compact = (c_i == r_i + (PAD - CAP) * q_i).astype(F32).astype(BF16)
    r_e = lax.broadcasted_iota(jnp.int32, (PADROWS, ROWS), 0)
    c_e = lax.broadcasted_iota(jnp.int32, (PADROWS, ROWS), 1)
    q_e = sum((c_e >= CAP * k).astype(jnp.int32) for k in (1, 2, 3))
    expand = (r_e == c_e + (PAD - CAP) * q_e).astype(F32).astype(BF16)

    ag = [dict() for _ in range(NG)]

    def ag_copy(i, n, src, dst, tpi):
        cp = remote(src, dst, g_s.at[i, n], g_r.at[i, n], sp, tpi)
        cp.start()
        ag[i][n] = cp
        sends.append(cp)

    def gather1(i):
        blocks = []
        for j in range(4 * i, 4 * i + 4):
            if j == SELF:
                blocks.append(outg[j])
            else:
                acopies[j].wait_recv()
                blocks.append(arecv[j])
        own = jnp.dot(compact, jnp.concatenate(blocks, axis=0), preferred_element_type=F32)
        xbuf[i, 0, 0] = own.astype(BF16)
        src = xbuf.at[i, 0, 0]
        ag_copy(i, 0, src, xbuf.at[i, 0, 3], up)
        ag_copy(i, 1, src, xbuf.at[i, 0, 1], down)
        ag_copy(i, 2, src, xbuf.at[i, 1, 0], mate)

    lo, hi = pl.ds(0, HALF), pl.ds(HALF, HALF)

    def gather2(i):
        ag[i][0].wait_recv()
        ag_copy(i, 3, xbuf.at[i, 0, 3, :, lo], xbuf.at[i, 0, 2, :, lo], up)
        ag_copy(i, 6, xbuf.at[i, 0, 3], xbuf.at[i, 1, 3], mate)
        ag[i][1].wait_recv()
        ag_copy(i, 4, xbuf.at[i, 0, 1, :, hi], xbuf.at[i, 0, 2, :, hi], down)
        ag_copy(i, 5, xbuf.at[i, 0, 1], xbuf.at[i, 1, 1], mate)

    def gather3(i):
        ag[i][3].wait_recv()
        ag[i][4].wait_recv()
        ag_copy(i, 7, xbuf.at[i, 0, 2], xbuf.at[i, 1, 2], mate)
        for n in (2, 5, 6, 7):
            ag[i][n].wait_recv()

    rs = [dict() for _ in range(NG)]

    def rs_copy(i, n, src, dst, tpi):
        cp = remote(src, dst, s_s.at[i, n], s_r.at[i, n], sp, tpi)
        cp.start()
        rs[i][n] = cp
        sends.append(cp)

    def experts(i):
        if i == 0:
            for cp in wcopies[:14]:
                cp.wait()

        @pl.loop(0, 7)
        def _(j):
            gu = jnp.dot(xbuf[i].reshape(8 * ROWS, D), wgu[j], preferred_element_type=F32)
            g, u = gu[:, :128], gu[:, 128:]
            h = g * (1.0 / (1.0 + jnp.exp(-g))) * u
            hbuf[:, pl.ds(pl.multiple_of(j * 128, 128), 128)] = h.astype(BF16)

        if i == 0:
            wcopies[14].wait()
        for half in (1, 0):

            @pl.loop(0, 8)
            def _(n):
                cols = pl.ds(pl.multiple_of(n * 256, 256), 256)
                p = jnp.dot(
                    hbuf[4 * ROWS * half : 4 * ROWS * (half + 1), :],
                    wd[:, cols],
                    preferred_element_type=F32,
                )
                pbuf[i, half, :, :, cols] = p.astype(BF16).reshape(4, ROWS, 256)

            if half == 1:
                rs_copy(i, 0, pbuf.at[i, 1], precv.at[i], mate)

    def both(i, k, cols):
        return pbuf[i, 0, k, :, cols].astype(F32) + precv[i, k, :, cols].astype(F32)

    def scatter1(i):
        rs[i][0].wait_recv()
        pbuf[i, 0, 2] = both(i, 2, slice(None)).astype(BF16)
        rs_copy(i, 1, pbuf.at[i, 0, 2, :, lo], r1.at[i, 0], up)
        rs_copy(i, 2, pbuf.at[i, 0, 2, :, hi], r1.at[i, 1], down)
        pbuf[i, 0, 1, :, HALF:] = both(i, 1, slice(HALF, D)).astype(BF16)
        rs_copy(i, 3, pbuf.at[i, 0, 1, :, hi], r2.at[i, 0, :, hi], up)
        pbuf[i, 0, 3, :, :HALF] = both(i, 3, slice(0, HALF)).astype(BF16)
        rs_copy(i, 4, pbuf.at[i, 0, 3, :, lo], r2.at[i, 1, :, lo], down)

    def scatter2(i):
        rs[i][1].wait_recv()
        pbuf[i, 0, 1, :, :HALF] = (both(i, 1, slice(0, HALF)) + r1[i, 0].astype(F32)).astype(BF16)
        rs_copy(i, 5, pbuf.at[i, 0, 1, :, lo], r2.at[i, 0, :, lo], up)
        rs[i][2].wait_recv()
        pbuf[i, 0, 3, :, HALF:] = (both(i, 3, slice(HALF, D)) + r1[i, 1].astype(F32)).astype(BF16)
        rs_copy(i, 6, pbuf.at[i, 0, 3, :, hi], r2.at[i, 1, :, hi], down)

    tcopies = {}

    def give_back(i):
        for n in (3, 4, 5, 6):
            rs[i][n].wait_recv()
        total = both(i, 0, slice(None)) + r2[i, 0].astype(F32) + r2[i, 1].astype(F32)
        padded = jnp.dot(expand, total.astype(BF16), preferred_element_type=F32)
        padded = padded.astype(BF16).reshape(4, PAD, D)
        for q in range(4):
            j = 4 * i + q
            dz, dx = OFFS[j]
            if j == SELF:
                ret_r[j] = padded[q]
            else:
                ret_s[j] = padded[q]
                tcopies[j] = remote(
                    ret_s.at[j], ret_r.at[j], t_s.at[j], t_r.at[j], sp_at(4 - dz, 4 - dx), tp
                )
                tcopies[j].start()
                sends.append(tcopies[j])

    gather1(0)
    gather1(1)
    gather2(0)
    gather1(2)
    gather2(1)
    gather3(0)
    experts(0)
    scatter1(0)
    gather1(3)
    gather2(2)
    scatter2(0)
    gather3(1)
    experts(1)
    scatter1(1)
    gather2(3)
    scatter2(1)
    gather3(2)
    experts(2)
    scatter1(2)
    give_back(0)
    scatter2(2)
    gather3(3)
    experts(3)
    scatter1(3)
    give_back(1)
    scatter2(3)
    give_back(2)
    give_back(3)
    for j in range(16):
        if j != SELF:
            tcopies[j].wait_recv()
    ret = ret_r[...].reshape(16 * PAD, D)
    mix = jnp.dot(comb_ref[0], ret, preferred_element_type=F32)
    mix = mix + jnp.dot(comb_ref[1], ret, preferred_element_type=F32)
    scale = lax.rsqrt(jnp.mean(mix * mix, axis=1, keepdims=True) + 1e-06)
    out_ref[...] = (stream_ref[...] + mix * scale * gain_ref[...].astype(F32)).astype(BF16)
    for cp in sends:
        cp.wait_send()


def moe(normed, stream, disp, comb, gain, wg, wu, wd):
    vmem = pl.BlockSpec(memory_space=pltpu.VMEM)
    hbm = pl.BlockSpec(memory_space=pl.ANY)
    dma = pltpu.SemaphoreType.DMA
    return pl.pallas_call(
        moe_kernel,
        out_shape=jax.ShapeDtypeStruct((TOK, D), BF16),
        in_specs=[vmem] * 5 + [hbm] * 3,
        out_specs=vmem,
        scratch_shapes=[
            pltpu.VMEM((7, D, 256), BF16),
            pltpu.VMEM((FFB, D), BF16),
            pltpu.VMEM((16, PAD, D), BF16),
            pltpu.VMEM((16, PAD, D), BF16),
            pltpu.VMEM((NG, 2, 4, ROWS, D), BF16),
            pltpu.VMEM((8 * ROWS, FFB), BF16),
            pltpu.VMEM((NG, 2, 4, ROWS, D), BF16),
            pltpu.VMEM((NG, 4, ROWS, D), BF16),
            pltpu.VMEM((NG, 2, ROWS, HALF), BF16),
            pltpu.VMEM((NG, 2, ROWS, D), BF16),
            pltpu.VMEM((16, PAD, D), BF16),
            pltpu.VMEM((16, PAD, D), BF16),
            dma((15,)),
            dma((16,)),
            dma((16,)),
            dma((NG, 8)),
            dma((NG, 8)),
            dma((NG, 7)),
            dma((NG, 7)),
            dma((16,)),
            dma((16,)),
        ],
        compiler_params=pltpu.CompilerParams(
            collective_id=0, has_side_effects=True, vmem_limit_bytes=62 * 1024 * 1024
        ),
        name="moe",
    )(normed, stream, disp, comb, gain, wg, wu, wd)


def passed_along(value, axis, steps):
    count = lax.axis_size(axis)
    leading, last = (max(0, -steps), min(count, count - steps))
    return lax.ppermute(value, axis, [(source, source + steps) for source in range(leading, last)])


def copy_for_each(value, axis):
    copies = jnp.broadcast_to(value, (lax.axis_size(axis), *value.shape))
    return lax.all_to_all(copies, axis, split_axis=0, concat_axis=0, tiled=True)


def over_copies(value, axis):
    return copy_for_each(value, axis).sum(axis=0)


def together(arrays, axis):
    ends = [0]
    for a in arrays:
        ends.append(ends[-1] + a.size)
    subtotal = over_copies(jnp.concatenate([a.ravel() for a in arrays]), axis)
    return tuple((subtotal[b:e].reshape(a.shape) for a, b, e in zip(arrays, ends, ends[1:])))


def route_tables(routes, route_weights):
    sp = lax.axis_index("sp")
    z, x = sp // 4, sp % 4
    flat = routes.reshape(-1)
    experts = jnp.arange(16, dtype=jnp.int32)
    matches = (flat[:, None] == experts[None, :]).astype(jnp.int32)
    before = jnp.cumsum(matches, axis=0) - matches
    slot = jnp.sum(before * matches, axis=1)
    rel = ((flat // 4 - z) % 4) * 4 + (flat % 4 - x) % 4
    place = jnp.zeros_like(rel)
    for j, (dz, dx) in enumerate(OFFS):
        place = place + jnp.where(rel == dz * 4 + dx, j, 0)
    target = (place * PAD + slot).reshape(TOK, 2)
    slots = jnp.arange(16 * PAD, dtype=jnp.int32)
    disp = jnp.any(target.T[:, None, :] == slots[None, :, None], axis=0).astype(BF16)
    hits = target[:, :, None] == slots[None, None, :]
    comb = jnp.sum(jnp.where(hits, route_weights[:, :, None], 0.0), axis=1)
    high = comb.astype(BF16)
    low = (comb - high.astype(F32)).astype(BF16)
    return disp, jnp.stack([high, low])


def per_device(
    a_lin,
    a_gate,
    conv_weight,
    ln_gain,
    ln_bias,
    proj_weight,
    residual,
    mix_gain,
    ffn_gain,
    routes,
    route_weights,
    gate_weight,
    up_weight,
    down_weight,
    out_gain,
):
    kernel_len = conv_weight.shape[0]
    gated = (a_lin.astype(jnp.float32) * jax.nn.sigmoid(a_gate.astype(jnp.float32))).astype(
        jnp.bfloat16
    )
    row_count = gated.shape[0]
    edge_rows = passed_along(gated[row_count - (kernel_len - 1) :], "sp", 1)
    padded = jnp.concatenate([edge_rows, gated], 0).astype(jnp.float32)
    filter_taps = conv_weight.astype(jnp.float32)
    conv_out = filter_taps[0] * padded[0:row_count]
    for offset in range(1, kernel_len):
        conv_out = conv_out + filter_taps[offset] * padded[offset : offset + row_count]
    row_total, squares = together(
        (jnp.sum(conv_out, axis=1), jnp.sum(conv_out * conv_out, axis=1)), "tp"
    )
    row_mean = row_total / D_A
    row_var = squares / D_A - row_mean * row_mean
    scaled = (conv_out - row_mean[:, None]) * lax.rsqrt(row_var[:, None] + 1e-05)
    scaled = scaled * ln_gain.astype(jnp.float32) + ln_bias.astype(jnp.float32)
    activated = jax.nn.silu(scaled).astype(jnp.bfloat16)
    token_acts = lax.all_to_all(activated, "tp", split_axis=0, concat_axis=1, tiled=True)
    branch = jnp.dot(token_acts, proj_weight, preferred_element_type=jnp.float32)
    branch_f = lax.optimization_barrier(branch.astype(jnp.bfloat16)).astype(jnp.float32)
    branch_scale = lax.rsqrt(jnp.mean(branch_f * branch_f, axis=1, keepdims=True) + 1e-06)
    stream = residual.astype(jnp.float32) + branch_f * branch_scale * mix_gain.astype(jnp.float32)
    stream_scale = lax.rsqrt(jnp.mean(stream * stream, axis=1, keepdims=True) + 1e-06)
    normed = (stream * stream_scale * ffn_gain.astype(jnp.float32)).astype(jnp.bfloat16)
    disp, comb = route_tables(routes, route_weights)
    return moe(
        normed, stream, disp, comb, out_gain.reshape(1, D), gate_weight, up_weight, down_weight
    )


def solution(mesh):
    return jax.shard_map(
        per_device,
        mesh=mesh,
        in_specs=(
            P("sp", "tp"),
            P("sp", "tp"),
            P(None, "tp"),
            P("tp"),
            P("tp"),
            P(),
            P(("sp", "tp"), None),
            P(),
            P(),
            P(("sp", "tp"), None),
            P(("sp", "tp"), None),
            P("sp", None, "tp"),
            P("sp", None, "tp"),
            P("sp", "tp", None),
            P(),
        ),
        out_specs=P(("sp", "tp"), None),
        check_vma=False,
    )
```

```python
import jax
import jax.numpy as jnp
from jax import lax
from jax.experimental import pallas as pl
from jax.experimental.pallas import tpu as pltpu
from jax.sharding import PartitionSpec as P

D = 2048
D_A = 1024
HALF = D // 2
FFB = 896
CAP = 20
PAD = 24
TOK = 128
NG = 4
ROWS = 4 * CAP
PADROWS = 4 * PAD
EDGE = 32
MESH = pl.DeviceIdType.MESH
BF16 = jnp.bfloat16
F32 = jnp.float32

GROUPS = (
    ((0, 1), (0, 3), (1, 0), (3, 0)),
    ((0, 0), (0, 2), (2, 0), (2, 2)),
    ((2, 1), (2, 3), (1, 2), (3, 2)),
    ((1, 1), (1, 3), (3, 1), (3, 3)),
)
OFFS = tuple(o for g in GROUPS for o in g)
SELF = OFFS.index((0, 0))


def layer_kernel(
    lin_hbm,
    gate_hbm,
    taps_ref,
    proj_hbm,
    resid_hbm,
    gains_ref,
    routes_ref,
    rweights_ref,
    wg_hbm,
    wu_hbm,
    wd_hbm,
    out_ref,
    lin,
    gatein,
    resid,
    proj,
    gsrc,
    taps,
    gbuf,
    padf,
    conv,
    act,
    branch,
    stream_ref,
    normed_ref,
    comb_ref,
    disp_ref,
    wgu,
    wd,
    outg,
    arecv,
    xbuf,
    hbuf,
    pbuf,
    precv,
    r1,
    r2,
    ret_s,
    ret_r,
    isem,
    wsem,
    c_s,
    c_r,
    a_s,
    a_r,
    g_s,
    g_r,
    s_s,
    s_r,
    t_s,
    t_r,
):
    sp = lax.axis_index("sp")
    tp = lax.axis_index("tp")
    z, x = lax.div(sp, 4), lax.rem(sp, 4)
    y, c = lax.div(tp, 2), lax.rem(tp, 2)

    def sp_at(dz, dx):
        return lax.rem(z + dz, 4) * 4 + lax.rem(x + dx, 4)

    up = lax.rem(y + 1, 4) * 2 + c
    down = lax.rem(y + 3, 4) * 2 + c
    mate = y * 2 + 1 - c

    icopies = [
        pltpu.make_async_copy(src, dst, isem.at[n])
        for n, (src, dst) in enumerate(
            ((lin_hbm, lin), (gate_hbm, gatein), (resid_hbm, resid), (proj_hbm, proj))
        )
    ]
    for cp in icopies:
        cp.start()

    wcopies = []
    for j in range(7):
        cols = pl.ds(128 * j, 128)
        for h, w in enumerate((wg_hbm, wu_hbm)):
            wcopies.append(
                pltpu.make_async_copy(
                    w.at[0, :, cols], wgu.at[j, :, pl.ds(128 * h, 128)], wsem.at[2 * j + h]
                )
            )
    wcopies.append(pltpu.make_async_copy(wd_hbm.at[0], wd, wsem.at[14]))
    for cp in wcopies:
        cp.start()

    barrier = pltpu.get_barrier_semaphore()

    def greet(spi, tpi):
        pl.semaphore_signal(
            barrier, inc=1, device_id={"sp": spi, "tp": tpi}, device_id_type=MESH
        )

    for r in range(1, 8):
        greet(sp, lax.rem(tp + r, 8))
    for o in OFFS:
        if o != (0, 0):
            greet(sp_at(*o), tp)

    @pl.when(tp == 0)
    def _():
        for t in range(1, 8):
            greet(lax.rem(sp + 15, 16), t)

    icopies[0].wait()
    icopies[1].wait()
    for n in range(4):
        rows = pl.ds(256 * n, 256)
        g = gatein[rows, :].astype(F32)
        gsrc[rows, :] = (lin[rows, :].astype(F32) * (1.0 / (1.0 + jnp.exp(-g)))).astype(BF16)
    pl.semaphore_wait(barrier, 22 + jnp.minimum(tp, 1))

    def remote(src, dst, ssem, rsem, spi, tpi):
        return pltpu.make_async_remote_copy(
            src_ref=src,
            dst_ref=dst,
            send_sem=ssem,
            recv_sem=rsem,
            device_id={"sp": spi, "tp": tpi},
            device_id_type=MESH,
        )

    sends = []
    ccopies = []

    def exchange(n, src, dst, spi, tpi):
        cp = remote(src, dst, c_s.at[n], c_r.at[n], spi, tpi)
        cp.start()
        ccopies.append(cp)
        sends.append(cp)

    def edge_of(t):
        return pl.ds(pl.multiple_of(lax.rem(t + 7, 8) * TOK + TOK - EDGE, EDGE), EDGE)

    def body_of(t):
        return pl.ds(pl.multiple_of(t * TOK, TOK), TOK)

    for r in range(1, 8):
        t = lax.rem(tp + r, 8)
        exchange(r - 1, gsrc.at[body_of(t)], gbuf.at[tp, pl.ds(EDGE, TOK)], sp, t)
        first = lax.div(8 - t, 8)
        exchange(
            6 + r, gsrc.at[edge_of(t)], gbuf.at[tp, pl.ds(0, EDGE)], lax.rem(sp + first, 16), t
        )
    for r in range(1, 8):
        exchange(13 + r, taps_ref, taps.at[tp], sp, lax.rem(tp + r, 8))
    own_edge = remote(
        gsrc.at[edge_of(0)],
        gbuf.at[tp, pl.ds(0, EDGE)],
        c_s.at[21],
        c_r.at[21],
        lax.rem(sp + 1, 16),
        tp,
    )

    @pl.when(tp == 0)
    def _():
        own_edge.start()

    @pl.when(tp > 0)
    def _():
        gbuf[tp, 0:EDGE] = gsrc[edge_of(tp), :]

    gbuf[tp, EDGE:] = gsrc[body_of(tp), :]
    taps[tp] = taps_ref[...]

    lane = lax.broadcasted_iota(jnp.int32, (1, TOK), 1)
    code = lax.broadcasted_iota(jnp.int32, (16, TOK), 0)
    places, counts = [], jnp.zeros((16, TOK), F32)
    for k in range(2):
        e = routes_ref[k : k + 1, :]
        ez, ex = lax.shift_right_logical(e, 2), jnp.bitwise_and(e, 3)
        rel = jnp.bitwise_and(ez - z + 4, 3) * 4 + jnp.bitwise_and(ex - x + 4, 3)
        place = jnp.zeros_like(rel)
        for j, (dz, dx) in enumerate(OFFS):
            place = jnp.where(rel == dz * 4 + dx, j, place)
        places.append(place)
        counts = counts + jnp.where(code == place, 1.0, 0.0)
    earlier = lax.broadcasted_iota(jnp.int32, (TOK, TOK), 0) < lax.broadcasted_iota(
        jnp.int32, (TOK, TOK), 1
    )
    before = jnp.dot(
        counts.astype(BF16),
        jnp.where(earlier, 1.0, 0.0).astype(BF16),
        preferred_element_type=F32,
    )
    row = lax.broadcasted_iota(jnp.int32, (16 * PAD, TOK), 0)
    disp, comb = jnp.zeros((16 * PAD, TOK), F32), jnp.zeros((16 * PAD, TOK), F32)
    for k in range(2):
        slot = jnp.sum(jnp.where(code == places[k], before, 0.0), axis=0, keepdims=True)
        hit = row == places[k] * PAD + slot.astype(jnp.int32)
        disp = jnp.where(hit, 1.0, disp)
        comb = jnp.where(hit, rweights_ref[k : k + 1, :], comb)
    disp_ref[...] = disp.astype(BF16)
    comb = comb.T
    high = comb.astype(BF16)
    comb_ref[0] = high
    comb_ref[1] = (comb - high.astype(F32)).astype(BF16)

    for cp in ccopies:
        cp.wait_recv()

    @pl.when(tp == 0)
    def _():
        own_edge.wait_recv()

    no_edge = jnp.logical_and(sp == 0, tp == 0)
    keep = jnp.where(no_edge, 0.0, 1.0)
    edge_mask = jnp.where(lax.broadcasted_iota(jnp.int32, (EDGE + TOK, TOK), 0) < EDGE, keep, 1.0)

    def filtered(b, sums):
        padf[...] = gbuf[b].astype(F32) * edge_mask
        w = taps[b].astype(F32)
        total = w[0:1] * padf[2 : 2 + TOK, :]
        for k in range(1, 31):
            total = total + w[k : k + 1] * padf[2 + k : 2 + k + TOK, :]
        conv[b] = total
        return sums[0] + total, sums[1] + total * total

    zero = jnp.zeros((TOK, TOK), F32)
    sum1, sum2 = lax.fori_loop(0, 8, filtered, (zero, zero))
    mean = jnp.sum(sum1, axis=1, keepdims=True) / D_A
    var = jnp.sum(sum2, axis=1, keepdims=True) / D_A - mean * mean
    rstd = lax.rsqrt(var + 1e-05)

    @pl.loop(0, 8)
    def _(b):
        w = taps[b].astype(F32)
        v = (conv[b] - mean) * rstd * w[31:32] + w[32:33]
        act[:, pl.ds(pl.multiple_of(b * TOK, TOK), TOK)] = (v * (1.0 / (1.0 + jnp.exp(-v)))).astype(
            BF16
        )

    icopies[3].wait()

    @pl.loop(0, 8)
    def _(n):
        cols = pl.ds(pl.multiple_of(n * 256, 256), 256)
        branch[:, cols] = jnp.dot(act[...], proj[:, cols], preferred_element_type=F32).astype(BF16)

    icopies[2].wait()

    @pl.loop(0, 8)
    def _(n):
        rows = pl.ds(pl.multiple_of(n * 16, 16), 16)
        b = branch[rows, :].astype(F32)
        scale = lax.rsqrt(jnp.mean(b * b, axis=1, keepdims=True) + 1e-06)
        st = resid[rows, :].astype(F32) + b * scale * gains_ref[0:1, :]
        stream_ref[rows, :] = st
        scale = lax.rsqrt(jnp.mean(st * st, axis=1, keepdims=True) + 1e-06)
        normed_ref[rows, :] = (st * scale * gains_ref[1:2, :]).astype(BF16)

    acopies = {}
    for i in range(NG):
        rows = jnp.dot(
            disp_ref[PADROWS * i : PADROWS * (i + 1), :],
            normed_ref[...],
            preferred_element_type=F32,
        )
        outg[4 * i : 4 * i + 4] = rows.astype(BF16).reshape(4, PAD, D)
        for j in range(4 * i, 4 * i + 4):
            if j != SELF:
                acopies[j] = remote(
                    outg.at[j], arecv.at[j], a_s.at[j], a_r.at[j], sp_at(*OFFS[j]), tp
                )
                acopies[j].start()
                sends.append(acopies[j])

    r_i = lax.broadcasted_iota(jnp.int32, (ROWS, PADROWS), 0)
    c_i = lax.broadcasted_iota(jnp.int32, (ROWS, PADROWS), 1)
    q_i = sum((r_i >= CAP * k).astype(jnp.int32) for k in (1, 2, 3))
    compact = (c_i == r_i + (PAD - CAP) * q_i).astype(F32).astype(BF16)
    r_e = lax.broadcasted_iota(jnp.int32, (PADROWS, ROWS), 0)
    c_e = lax.broadcasted_iota(jnp.int32, (PADROWS, ROWS), 1)
    q_e = sum((c_e >= CAP * k).astype(jnp.int32) for k in (1, 2, 3))
    expand = (r_e == c_e + (PAD - CAP) * q_e).astype(F32).astype(BF16)

    ag = [dict() for _ in range(NG)]

    def ag_copy(i, n, src, dst, tpi):
        cp = remote(src, dst, g_s.at[i, n], g_r.at[i, n], sp, tpi)
        cp.start()
        ag[i][n] = cp
        sends.append(cp)

    def gather1(i):
        blocks = []
        for j in range(4 * i, 4 * i + 4):
            if j == SELF:
                blocks.append(outg[j])
            else:
                acopies[j].wait_recv()
                blocks.append(arecv[j])
        own = jnp.dot(compact, jnp.concatenate(blocks, axis=0), preferred_element_type=F32)
        xbuf[i, 0, 0] = own.astype(BF16)
        src = xbuf.at[i, 0, 0]
        ag_copy(i, 0, src, xbuf.at[i, 0, 3], up)
        ag_copy(i, 1, src, xbuf.at[i, 0, 1], down)
        ag_copy(i, 2, src, xbuf.at[i, 1, 0], mate)

    lo, hi = pl.ds(0, HALF), pl.ds(HALF, HALF)

    def gather2(i):
        ag[i][0].wait_recv()
        ag_copy(i, 3, xbuf.at[i, 0, 3, :, lo], xbuf.at[i, 0, 2, :, lo], up)
        ag_copy(i, 6, xbuf.at[i, 0, 3], xbuf.at[i, 1, 3], mate)
        ag[i][1].wait_recv()
        ag_copy(i, 4, xbuf.at[i, 0, 1, :, hi], xbuf.at[i, 0, 2, :, hi], down)
        ag_copy(i, 5, xbuf.at[i, 0, 1], xbuf.at[i, 1, 1], mate)

    def gather3(i):
        ag[i][3].wait_recv()
        ag[i][4].wait_recv()
        ag_copy(i, 7, xbuf.at[i, 0, 2], xbuf.at[i, 1, 2], mate)
        for n in (2, 5, 6, 7):
            ag[i][n].wait_recv()

    rs = [dict() for _ in range(NG)]

    def rs_copy(i, n, src, dst, tpi):
        cp = remote(src, dst, s_s.at[i, n], s_r.at[i, n], sp, tpi)
        cp.start()
        rs[i][n] = cp
        sends.append(cp)

    def experts(i):
        if i == 0:
            for cp in wcopies[:14]:
                cp.wait()

        @pl.loop(0, 7)
        def _(j):
            gu = jnp.dot(xbuf[i].reshape(8 * ROWS, D), wgu[j], preferred_element_type=F32)
            g, u = gu[:, :128], gu[:, 128:]
            h = g * (1.0 / (1.0 + jnp.exp(-g))) * u
            hbuf[:, pl.ds(pl.multiple_of(j * 128, 128), 128)] = h.astype(BF16)

        if i == 0:
            wcopies[14].wait()
        for half in (1, 0):

            @pl.loop(0, 8)
            def _(n):
                cols = pl.ds(pl.multiple_of(n * 256, 256), 256)
                p = jnp.dot(
                    hbuf[4 * ROWS * half : 4 * ROWS * (half + 1), :],
                    wd[:, cols],
                    preferred_element_type=F32,
                )
                pbuf[i, half, :, :, cols] = p.astype(BF16).reshape(4, ROWS, 256)

            if half == 1:
                rs_copy(i, 0, pbuf.at[i, 1], precv.at[i], mate)

    def both(i, k, cols):
        return pbuf[i, 0, k, :, cols].astype(F32) + precv[i, k, :, cols].astype(F32)

    def scatter1(i):
        rs[i][0].wait_recv()
        pbuf[i, 0, 2] = both(i, 2, slice(None)).astype(BF16)
        rs_copy(i, 1, pbuf.at[i, 0, 2, :, lo], r1.at[i, 0], up)
        rs_copy(i, 2, pbuf.at[i, 0, 2, :, hi], r1.at[i, 1], down)
        pbuf[i, 0, 1, :, HALF:] = both(i, 1, slice(HALF, D)).astype(BF16)
        rs_copy(i, 3, pbuf.at[i, 0, 1, :, hi], r2.at[i, 0, :, hi], up)
        pbuf[i, 0, 3, :, :HALF] = both(i, 3, slice(0, HALF)).astype(BF16)
        rs_copy(i, 4, pbuf.at[i, 0, 3, :, lo], r2.at[i, 1, :, lo], down)

    def scatter2(i):
        rs[i][1].wait_recv()
        pbuf[i, 0, 1, :, :HALF] = (both(i, 1, slice(0, HALF)) + r1[i, 0].astype(F32)).astype(BF16)
        rs_copy(i, 5, pbuf.at[i, 0, 1, :, lo], r2.at[i, 0, :, lo], up)
        rs[i][2].wait_recv()
        pbuf[i, 0, 3, :, HALF:] = (both(i, 3, slice(HALF, D)) + r1[i, 1].astype(F32)).astype(BF16)
        rs_copy(i, 6, pbuf.at[i, 0, 3, :, hi], r2.at[i, 1, :, hi], down)

    tcopies = {}

    def give_back(i):
        for n in (3, 4, 5, 6):
            rs[i][n].wait_recv()
        total = both(i, 0, slice(None)) + r2[i, 0].astype(F32) + r2[i, 1].astype(F32)
        padded = jnp.dot(expand, total.astype(BF16), preferred_element_type=F32)
        padded = padded.astype(BF16).reshape(4, PAD, D)
        for q in range(4):
            j = 4 * i + q
            dz, dx = OFFS[j]
            if j == SELF:
                ret_r[j] = padded[q]
            else:
                ret_s[j] = padded[q]
                tcopies[j] = remote(
                    ret_s.at[j], ret_r.at[j], t_s.at[j], t_r.at[j], sp_at(4 - dz, 4 - dx), tp
                )
                tcopies[j].start()
                sends.append(tcopies[j])

    gather1(0)
    gather1(1)
    gather2(0)
    gather1(2)
    gather2(1)
    gather3(0)
    experts(0)
    scatter1(0)
    gather1(3)
    gather2(2)
    scatter2(0)
    gather3(1)
    experts(1)
    scatter1(1)
    gather2(3)
    scatter2(1)
    gather3(2)
    experts(2)
    scatter1(2)
    give_back(0)
    scatter2(2)
    gather3(3)
    experts(3)
    scatter1(3)
    give_back(1)
    scatter2(3)
    give_back(2)
    give_back(3)
    for j in range(16):
        if j != SELF:
            tcopies[j].wait_recv()
    ret = ret_r[...].reshape(16 * PAD, D)
    mix = jnp.dot(comb_ref[0], ret, preferred_element_type=F32)
    mix = mix + jnp.dot(comb_ref[1], ret, preferred_element_type=F32)
    scale = lax.rsqrt(jnp.mean(mix * mix, axis=1, keepdims=True) + 1e-06)
    out_ref[...] = (stream_ref[...] + mix * scale * gains_ref[2:3, :]).astype(BF16)
    for cp in sends:
        cp.wait_send()

    @pl.when(tp == 0)
    def _():
        own_edge.wait_send()


def layer(*operands):
    vmem = pl.BlockSpec(memory_space=pltpu.VMEM)
    hbm = pl.BlockSpec(memory_space=pl.ANY)
    dma = pltpu.SemaphoreType.DMA
    return pl.pallas_call(
        layer_kernel,
        out_shape=jax.ShapeDtypeStruct((TOK, D), BF16),
        in_specs=[hbm, hbm, vmem, hbm, hbm, vmem, vmem, vmem, hbm, hbm, hbm],
        out_specs=vmem,
        scratch_shapes=[
            pltpu.VMEM((8 * TOK, TOK), BF16),
            pltpu.VMEM((8 * TOK, TOK), BF16),
            pltpu.VMEM((TOK, D), BF16),
            pltpu.VMEM((D_A, D), BF16),
            pltpu.VMEM((8 * TOK, TOK), BF16),
            pltpu.VMEM((8, 48, TOK), BF16),
            pltpu.VMEM((8, EDGE + TOK, TOK), BF16),
            pltpu.VMEM((EDGE + TOK, TOK), F32),
            pltpu.VMEM((8, TOK, TOK), F32),
            pltpu.VMEM((TOK, D_A), BF16),
            pltpu.VMEM((TOK, D), BF16),
            pltpu.VMEM((TOK, D), F32),
            pltpu.VMEM((TOK, D), BF16),
            pltpu.VMEM((2, TOK, 16 * PAD), BF16),
            pltpu.VMEM((16 * PAD, TOK), BF16),
            pltpu.VMEM((7, D, 256), BF16),
            pltpu.VMEM((FFB, D), BF16),
            pltpu.VMEM((16, PAD, D), BF16),
            pltpu.VMEM((16, PAD, D), BF16),
            pltpu.VMEM((NG, 2, 4, ROWS, D), BF16),
            pltpu.VMEM((8 * ROWS, FFB), BF16),
            pltpu.VMEM((NG, 2, 4, ROWS, D), BF16),
            pltpu.VMEM((NG, 4, ROWS, D), BF16),
            pltpu.VMEM((NG, 2, ROWS, HALF), BF16),
            pltpu.VMEM((NG, 2, ROWS, D), BF16),
            pltpu.VMEM((16, PAD, D), BF16),
            pltpu.VMEM((16, PAD, D), BF16),
            dma((4,)),
            dma((15,)),
            dma((22,)),
            dma((22,)),
            dma((16,)),
            dma((16,)),
            dma((NG, 8)),
            dma((NG, 8)),
            dma((NG, 7)),
            dma((NG, 7)),
            dma((16,)),
            dma((16,)),
        ],
        compiler_params=pltpu.CompilerParams(
            collective_id=0, has_side_effects=True, vmem_limit_bytes=62 * 1024 * 1024
        ),
        name="layer",
    )(*operands)


def per_device(
    a_lin,
    a_gate,
    conv_weight,
    ln_gain,
    ln_bias,
    proj_weight,
    residual,
    mix_gain,
    ffn_gain,
    routes,
    route_weights,
    gate_weight,
    up_weight,
    down_weight,
    out_gain,
):
    taps = jnp.concatenate(
        [conv_weight, ln_gain[None, :], ln_bias[None, :], jnp.zeros((15, TOK), BF16)], axis=0
    )
    gains = jnp.stack([mix_gain, ffn_gain, out_gain]).astype(F32)
    return layer(
        a_lin,
        a_gate,
        taps,
        proj_weight,
        residual,
        gains,
        routes.T,
        route_weights.T,
        gate_weight,
        up_weight,
        down_weight,
    )


def solution(mesh):
    return jax.shard_map(
        per_device,
        mesh=mesh,
        in_specs=(
            P("sp", "tp"),
            P("sp", "tp"),
            P(None, "tp"),
            P("tp"),
            P("tp"),
            P(),
            P(("sp", "tp"), None),
            P(),
            P(),
            P(("sp", "tp"), None),
            P(("sp", "tp"), None),
            P("sp", None, "tp"),
            P("sp", None, "tp"),
            P("sp", "tp", None),
            P(),
        ),
        out_specs=P(("sp", "tp"), None),
        check_vma=False,
    )
```

```python
import jax
import jax.numpy as jnp
from jax import lax
from jax.experimental import pallas as pl
from jax.experimental.pallas import tpu as pltpu
from jax.sharding import PartitionSpec as P

D = 2048
D_A = 1024
HALF = D // 2
FFB = 896
CAP = 20
PAD = 24
TOK = 128
NG = 4
DN = 1024
ROWS = 4 * CAP
PADROWS = 4 * PAD
EDGE = 32
MESH = pl.DeviceIdType.MESH
BF16 = jnp.bfloat16
F32 = jnp.float32

GROUPS = (
    ((1, 1), (1, 3), (3, 1), (3, 3)),
    ((0, 0), (0, 2), (2, 0), (2, 2)),
    ((2, 1), (2, 3), (1, 2), (3, 2)),
    ((0, 1), (0, 3), (1, 0), (3, 0)),
)
OFFS = tuple(o for g in GROUPS for o in g)
SELF = OFFS.index((0, 0))


def layer_kernel(
    lin_hbm,
    gate_hbm,
    conv_ref,
    lng_ref,
    lnb_ref,
    proj_hbm,
    resid_hbm,
    mixg_ref,
    ffng_ref,
    outg_ref,
    routes_ref,
    rweights_ref,
    wg_hbm,
    wu_hbm,
    wd_hbm,
    out_ref,
    lin,
    gatein,
    resid,
    proj,
    gsrc,
    small,
    taps,
    gbuf,
    padf,
    conv,
    act,
    branch,
    stream_ref,
    normed_ref,
    comb_ref,
    disp_ref,
    wgu,
    wd,
    outg,
    arecv,
    xbuf,
    hbuf,
    pbuf,
    precv,
    r1,
    r2,
    ret_s,
    ret_r,
    isem,
    wsem,
    c_s,
    c_r,
    a_s,
    a_r,
    g_s,
    g_r,
    s_s,
    s_r,
    t_s,
    t_r,
):
    sp = lax.axis_index("sp")
    tp = lax.axis_index("tp")
    z, x = lax.div(sp, 4), lax.rem(sp, 4)
    y, c = lax.div(tp, 2), lax.rem(tp, 2)

    def sp_at(dz, dx):
        return lax.rem(z + dz, 4) * 4 + lax.rem(x + dx, 4)

    up = lax.rem(y + 1, 4) * 2 + c
    down = lax.rem(y + 3, 4) * 2 + c
    mate = y * 2 + 1 - c

    icopies = [
        pltpu.make_async_copy(src, dst, isem.at[n])
        for n, (src, dst) in enumerate(
            ((lin_hbm, lin), (gate_hbm, gatein), (resid_hbm, resid), (proj_hbm, proj))
        )
    ]
    icopies[0].start()
    icopies[1].start()

    barrier = pltpu.get_barrier_semaphore()

    def greet(spi, tpi):
        pl.semaphore_signal(
            barrier, inc=1, device_id={"sp": spi, "tp": tpi}, device_id_type=MESH
        )

    for r in range(1, 8):
        greet(sp, lax.rem(tp + r, 8))
    for o in OFFS:
        if o != (0, 0):
            greet(sp_at(*o), tp)

    @pl.when(tp == 0)
    def _():
        for t in range(1, 8):
            greet(lax.rem(sp + 15, 16), t)

    def remote(src, dst, ssem, rsem, spi, tpi):
        return pltpu.make_async_remote_copy(
            src_ref=src,
            dst_ref=dst,
            send_sem=ssem,
            recv_sem=rsem,
            device_id={"sp": spi, "tp": tpi},
            device_id_type=MESH,
        )

    sends = []
    ccopies = []

    def exchange(n, src, dst, spi, tpi):
        cp = remote(src, dst, c_s.at[n], c_r.at[n], spi, tpi)
        cp.start()
        ccopies.append(cp)
        sends.append(cp)

    def edge_of(t):
        return pl.ds(pl.multiple_of(lax.rem(t + 7, 8) * TOK + TOK - EDGE, EDGE), EDGE)

    def body_of(t):
        return pl.ds(pl.multiple_of(t * TOK, TOK), TOK)

    small[...] = jnp.zeros((48, TOK), BF16)
    small[0:31] = conv_ref[...]
    small[31:32] = lng_ref[...].reshape(1, TOK)
    small[32:33] = lnb_ref[...].reshape(1, TOK)
    taps[tp] = small[...]
    icopies[0].wait()
    icopies[1].wait()
    wcopies = []
    for j in range(7):
        cols = pl.ds(128 * j, 128)
        for h, w in enumerate((wg_hbm, wu_hbm)):
            wcopies.append(
                pltpu.make_async_copy(
                    w.at[0, :, cols], wgu.at[j, :, pl.ds(128 * h, 128)], wsem.at[2 * j + h]
                )
            )
    wcopies.append(pltpu.make_async_copy(wd_hbm.at[0], wd, wsem.at[14]))
    for cp in icopies[2:] + wcopies:
        cp.start()


    def gate(t):
        g = gatein[body_of(t), :].astype(F32)
        v = lin[body_of(t), :].astype(F32) * (1.0 / (1.0 + jnp.exp(-g)))
        gsrc[body_of(t), :] = v.astype(BF16)

    gate(tp)
    gate(lax.rem(tp + 1, 8))
    pl.semaphore_wait(barrier, 22 + jnp.minimum(tp, 1))
    for r in range(1, 8):
        exchange(13 + r, small, taps.at[tp], sp, lax.rem(tp + r, 8))
    for r in range(1, 8):
        t = lax.rem(tp + r, 8)
        if r > 1:
            gate(t)
        exchange(r - 1, gsrc.at[body_of(t)], gbuf.at[tp, pl.ds(EDGE, TOK)], sp, t)
        first = lax.div(8 - t, 8)
        exchange(
            6 + r, gsrc.at[edge_of(t)], gbuf.at[tp, pl.ds(0, EDGE)], lax.rem(sp + first, 16), t
        )
    own_edge = remote(
        gsrc.at[edge_of(0)],
        gbuf.at[tp, pl.ds(0, EDGE)],
        c_s.at[21],
        c_r.at[21],
        lax.rem(sp + 1, 16),
        tp,
    )

    @pl.when(tp == 0)
    def _():
        own_edge.start()

    @pl.when(tp > 0)
    def _():
        gbuf[tp, 0:EDGE] = gsrc[edge_of(tp), :]

    gbuf[tp, EDGE:] = gsrc[body_of(tp), :]

    lane = lax.broadcasted_iota(jnp.int32, (1, TOK), 1)
    code = lax.broadcasted_iota(jnp.int32, (16, TOK), 0)
    places, counts = [], jnp.zeros((16, TOK), F32)
    for k in range(2):
        e = routes_ref[k : k + 1, :]
        ez, ex = lax.shift_right_logical(e, 2), jnp.bitwise_and(e, 3)
        rel = jnp.bitwise_and(ez - z + 4, 3) * 4 + jnp.bitwise_and(ex - x + 4, 3)
        place = jnp.zeros_like(rel)
        for j, (dz, dx) in enumerate(OFFS):
            place = jnp.where(rel == dz * 4 + dx, j, place)
        places.append(place)
        counts = counts + jnp.where(code == place, 1.0, 0.0)
    earlier = lax.broadcasted_iota(jnp.int32, (TOK, TOK), 0) < lax.broadcasted_iota(
        jnp.int32, (TOK, TOK), 1
    )
    before = jnp.dot(
        counts.astype(BF16),
        jnp.where(earlier, 1.0, 0.0).astype(BF16),
        preferred_element_type=F32,
    )
    row = lax.broadcasted_iota(jnp.int32, (16 * PAD, TOK), 0)
    disp, comb = jnp.zeros((16 * PAD, TOK), F32), jnp.zeros((16 * PAD, TOK), F32)
    for k in range(2):
        slot = jnp.sum(jnp.where(code == places[k], before, 0.0), axis=0, keepdims=True)
        hit = row == places[k] * PAD + slot.astype(jnp.int32)
        disp = jnp.where(hit, 1.0, disp)
        comb = jnp.where(hit, rweights_ref[k : k + 1, :], comb)
    disp_ref[...] = disp.astype(BF16)
    comb = comb.T
    high = comb.astype(BF16)
    comb_ref[0] = high
    comb_ref[1] = (comb - high.astype(F32)).astype(BF16)

    for cp in ccopies:
        cp.wait_recv()

    @pl.when(tp == 0)
    def _():
        own_edge.wait_recv()

    no_edge = jnp.logical_and(sp == 0, tp == 0)
    keep = jnp.where(no_edge, 0.0, 1.0)
    edge_mask = jnp.where(lax.broadcasted_iota(jnp.int32, (EDGE + TOK, TOK), 0) < EDGE, keep, 1.0)

    def filtered(b, sums):
        padf[...] = gbuf[b].astype(F32) * edge_mask
        w = taps[b].astype(F32)
        total = w[0:1] * padf[2 : 2 + TOK, :]
        for k in range(1, 31):
            total = total + w[k : k + 1] * padf[2 + k : 2 + k + TOK, :]
        conv[b] = total
        return sums[0] + total, sums[1] + total * total

    zero = jnp.zeros((TOK, TOK), F32)
    sum1, sum2 = lax.fori_loop(0, 8, filtered, (zero, zero))
    mean = jnp.sum(sum1, axis=1, keepdims=True) / D_A
    var = jnp.sum(sum2, axis=1, keepdims=True) / D_A - mean * mean
    rstd = lax.rsqrt(var + 1e-05)

    @pl.loop(0, 8)
    def _(b):
        w = taps[b].astype(F32)
        v = (conv[b] - mean) * rstd * w[31:32] + w[32:33]
        act[:, pl.ds(pl.multiple_of(b * TOK, TOK), TOK)] = (v * (1.0 / (1.0 + jnp.exp(-v)))).astype(
            BF16
        )

    icopies[3].wait()

    @pl.loop(0, 2)
    def _(n):
        cols = pl.ds(pl.multiple_of(n * 1024, 1024), 1024)
        branch[:, cols] = jnp.dot(act[...], proj[:, cols], preferred_element_type=F32).astype(BF16)

    icopies[2].wait()
    mixg = mixg_ref[...].astype(F32).reshape(1, D)
    ffng = ffng_ref[...].astype(F32).reshape(1, D)

    @pl.loop(0, 4)
    def _(n):
        rows = pl.ds(pl.multiple_of(n * 32, 32), 32)
        b = branch[rows, :].astype(F32)
        scale = lax.rsqrt(jnp.mean(b * b, axis=1, keepdims=True) + 1e-06)
        st = resid[rows, :].astype(F32) + b * scale * mixg
        stream_ref[rows, :] = st
        scale = lax.rsqrt(jnp.mean(st * st, axis=1, keepdims=True) + 1e-06)
        normed_ref[rows, :] = (st * scale * ffng).astype(BF16)

    acopies = {}
    for i in range(NG):
        rows = jnp.dot(
            disp_ref[PADROWS * i : PADROWS * (i + 1), :],
            normed_ref[...],
            preferred_element_type=F32,
        )
        outg[4 * i : 4 * i + 4] = rows.astype(BF16).reshape(4, PAD, D)
        for j in range(4 * i, 4 * i + 4):
            if j != SELF:
                acopies[j] = remote(
                    outg.at[j], arecv.at[j], a_s.at[j], a_r.at[j], sp_at(*OFFS[j]), tp
                )
                acopies[j].start()
                sends.append(acopies[j])

    r_i = lax.broadcasted_iota(jnp.int32, (ROWS, PADROWS), 0)
    c_i = lax.broadcasted_iota(jnp.int32, (ROWS, PADROWS), 1)
    q_i = sum((r_i >= CAP * k).astype(jnp.int32) for k in (1, 2, 3))
    compact = (c_i == r_i + (PAD - CAP) * q_i).astype(F32).astype(BF16)
    r_e = lax.broadcasted_iota(jnp.int32, (PADROWS, ROWS), 0)
    c_e = lax.broadcasted_iota(jnp.int32, (PADROWS, ROWS), 1)
    q_e = sum((c_e >= CAP * k).astype(jnp.int32) for k in (1, 2, 3))
    expand = (r_e == c_e + (PAD - CAP) * q_e).astype(F32).astype(BF16)

    ag = [dict() for _ in range(NG)]

    def ag_copy(i, n, src, dst, tpi):
        cp = remote(src, dst, g_s.at[i, n], g_r.at[i, n], sp, tpi)
        cp.start()
        ag[i][n] = cp
        sends.append(cp)

    def gather1(i):
        blocks = []
        for j in range(4 * i, 4 * i + 4):
            if j == SELF:
                blocks.append(outg[j])
            else:
                acopies[j].wait_recv()
                blocks.append(arecv[j])
        own = jnp.dot(compact, jnp.concatenate(blocks, axis=0), preferred_element_type=F32)
        xbuf[i, 0, 0] = own.astype(BF16)
        src = xbuf.at[i, 0, 0]
        ag_copy(i, 0, src, xbuf.at[i, 0, 3], up)
        ag_copy(i, 1, src, xbuf.at[i, 0, 1], down)
        ag_copy(i, 2, src, xbuf.at[i, 1, 0], mate)

    lo, hi = pl.ds(0, HALF), pl.ds(HALF, HALF)

    def gather2(i):
        ag[i][0].wait_recv()
        ag_copy(i, 3, xbuf.at[i, 0, 3, :, lo], xbuf.at[i, 0, 2, :, lo], up)
        ag_copy(i, 6, xbuf.at[i, 0, 3], xbuf.at[i, 1, 3], mate)
        ag[i][1].wait_recv()
        ag_copy(i, 4, xbuf.at[i, 0, 1, :, hi], xbuf.at[i, 0, 2, :, hi], down)
        ag_copy(i, 5, xbuf.at[i, 0, 1], xbuf.at[i, 1, 1], mate)

    def gather3(i):
        ag[i][3].wait_recv()
        ag[i][4].wait_recv()
        ag_copy(i, 7, xbuf.at[i, 0, 2], xbuf.at[i, 1, 2], mate)
        for n in (2, 5, 6, 7):
            ag[i][n].wait_recv()

    rs = [dict() for _ in range(NG)]

    def rs_copy(i, n, src, dst, tpi):
        cp = remote(src, dst, s_s.at[i, n], s_r.at[i, n], sp, tpi)
        cp.start()
        rs[i][n] = cp
        sends.append(cp)

    def hidden(i):
        if i == 0:
            for cp in wcopies[:14]:
                cp.wait()

        @pl.loop(0, 7)
        def _(j):
            gu = jnp.dot(xbuf[i].reshape(8 * ROWS, D), wgu[j], preferred_element_type=F32)
            g, u = gu[:, :128], gu[:, 128:]
            h = g * (1.0 / (1.0 + jnp.exp(-g))) * u
            hbuf[:, pl.ds(pl.multiple_of(j * 128, 128), 128)] = h.astype(BF16)

    def partial(i):
        if i == 0:
            wcopies[14].wait()
        for half in (1, 0):

            @pl.loop(0, D // DN)
            def _(n):
                cols = pl.ds(pl.multiple_of(n * DN, DN), DN)
                p = jnp.dot(
                    hbuf[4 * ROWS * half : 4 * ROWS * (half + 1), :],
                    wd[:, cols],
                    preferred_element_type=F32,
                )
                pbuf[i, half, :, :, cols] = p.astype(BF16).reshape(4, ROWS, DN)

            if half == 1:
                rs_copy(i, 0, pbuf.at[i, 1], precv.at[i], mate)

    def both(i, k, cols):
        return pbuf[i, 0, k, :, cols].astype(F32) + precv[i, k, :, cols].astype(F32)

    def scatter1(i):
        rs[i][0].wait_recv()
        pbuf[i, 0, 2] = both(i, 2, slice(None)).astype(BF16)
        rs_copy(i, 1, pbuf.at[i, 0, 2, :, lo], r1.at[i, 0], up)
        rs_copy(i, 2, pbuf.at[i, 0, 2, :, hi], r1.at[i, 1], down)
        pbuf[i, 0, 1, :, HALF:] = both(i, 1, slice(HALF, D)).astype(BF16)
        rs_copy(i, 3, pbuf.at[i, 0, 1, :, hi], r2.at[i, 0, :, hi], up)
        pbuf[i, 0, 3, :, :HALF] = both(i, 3, slice(0, HALF)).astype(BF16)
        rs_copy(i, 4, pbuf.at[i, 0, 3, :, lo], r2.at[i, 1, :, lo], down)

    def scatter2(i):
        rs[i][1].wait_recv()
        pbuf[i, 0, 1, :, :HALF] = (both(i, 1, slice(0, HALF)) + r1[i, 0].astype(F32)).astype(BF16)
        rs_copy(i, 5, pbuf.at[i, 0, 1, :, lo], r2.at[i, 0, :, lo], up)
        rs[i][2].wait_recv()
        pbuf[i, 0, 3, :, HALF:] = (both(i, 3, slice(HALF, D)) + r1[i, 1].astype(F32)).astype(BF16)
        rs_copy(i, 6, pbuf.at[i, 0, 3, :, hi], r2.at[i, 1, :, hi], down)

    tcopies = {}

    def give_back(i):
        for n in (3, 4, 5, 6):
            rs[i][n].wait_recv()
        total = both(i, 0, slice(None)) + r2[i, 0].astype(F32) + r2[i, 1].astype(F32)
        padded = jnp.dot(expand, total.astype(BF16), preferred_element_type=F32)
        padded = padded.astype(BF16).reshape(4, PAD, D)
        for q in range(4):
            j = 4 * i + q
            dz, dx = OFFS[j]
            if j == SELF:
                ret_r[j] = padded[q]
            else:
                ret_s[j] = padded[q]
                tcopies[j] = remote(
                    ret_s.at[j], ret_r.at[j], t_s.at[j], t_r.at[j], sp_at(4 - dz, 4 - dx), tp
                )
                tcopies[j].start()
                sends.append(tcopies[j])

    gather1(0)
    gather1(1)
    gather2(0)
    gather1(2)
    gather2(1)
    gather3(0)
    hidden(0)
    partial(0)
    gather1(3)
    gather2(2)
    scatter1(0)
    gather3(1)
    hidden(1)
    scatter2(0)
    gather2(3)
    partial(1)
    scatter1(1)
    gather3(2)
    hidden(2)
    scatter2(1)
    give_back(0)
    partial(2)
    scatter1(2)
    gather3(3)
    hidden(3)
    scatter2(2)
    give_back(1)
    partial(3)
    scatter1(3)
    give_back(2)
    scatter2(3)
    give_back(3)
    for j in range(16):
        if j != SELF:
            tcopies[j].wait_recv()
    ret = ret_r[...].reshape(16 * PAD, D)
    mix = jnp.dot(comb_ref[0], ret, preferred_element_type=F32)
    mix = mix + jnp.dot(comb_ref[1], ret, preferred_element_type=F32)
    scale = lax.rsqrt(jnp.mean(mix * mix, axis=1, keepdims=True) + 1e-06)
    out_ref[...] = (stream_ref[...] + mix * scale * outg_ref[...].astype(F32).reshape(1, D)).astype(BF16)
    for cp in sends:
        cp.wait_send()

    @pl.when(tp == 0)
    def _():
        own_edge.wait_send()


def layer(*operands):
    vmem = pl.BlockSpec(memory_space=pltpu.VMEM)
    hbm = pl.BlockSpec(memory_space=pl.ANY)
    dma = pltpu.SemaphoreType.DMA
    return pl.pallas_call(
        layer_kernel,
        out_shape=jax.ShapeDtypeStruct((TOK, D), BF16),
        in_specs=[hbm, hbm, vmem, vmem, vmem, hbm, hbm, vmem, vmem, vmem, vmem, vmem, hbm, hbm, hbm],
        out_specs=vmem,
        scratch_shapes=[
            pltpu.VMEM((8 * TOK, TOK), BF16),
            pltpu.VMEM((8 * TOK, TOK), BF16),
            pltpu.VMEM((TOK, D), BF16),
            pltpu.VMEM((D_A, D), BF16),
            pltpu.VMEM((8 * TOK, TOK), BF16),
            pltpu.VMEM((48, TOK), BF16),
            pltpu.VMEM((8, 48, TOK), BF16),
            pltpu.VMEM((8, EDGE + TOK, TOK), BF16),
            pltpu.VMEM((EDGE + TOK, TOK), F32),
            pltpu.VMEM((8, TOK, TOK), F32),
            pltpu.VMEM((TOK, D_A), BF16),
            pltpu.VMEM((TOK, D), BF16),
            pltpu.VMEM((TOK, D), F32),
            pltpu.VMEM((TOK, D), BF16),
            pltpu.VMEM((2, TOK, 16 * PAD), BF16),
            pltpu.VMEM((16 * PAD, TOK), BF16),
            pltpu.VMEM((7, D, 256), BF16),
            pltpu.VMEM((FFB, D), BF16),
            pltpu.VMEM((16, PAD, D), BF16),
            pltpu.VMEM((16, PAD, D), BF16),
            pltpu.VMEM((NG, 2, 4, ROWS, D), BF16),
            pltpu.VMEM((8 * ROWS, FFB), BF16),
            pltpu.VMEM((NG, 2, 4, ROWS, D), BF16),
            pltpu.VMEM((NG, 4, ROWS, D), BF16),
            pltpu.VMEM((NG, 2, ROWS, HALF), BF16),
            pltpu.VMEM((NG, 2, ROWS, D), BF16),
            pltpu.VMEM((16, PAD, D), BF16),
            pltpu.VMEM((16, PAD, D), BF16),
            dma((4,)),
            dma((15,)),
            dma((22,)),
            dma((22,)),
            dma((16,)),
            dma((16,)),
            dma((NG, 8)),
            dma((NG, 8)),
            dma((NG, 7)),
            dma((NG, 7)),
            dma((16,)),
            dma((16,)),
        ],
        compiler_params=pltpu.CompilerParams(
            collective_id=0, has_side_effects=True, vmem_limit_bytes=62 * 1024 * 1024
        ),
        name="layer",
    )(*operands)


def per_device(
    a_lin,
    a_gate,
    conv_weight,
    ln_gain,
    ln_bias,
    proj_weight,
    residual,
    mix_gain,
    ffn_gain,
    routes,
    route_weights,
    gate_weight,
    up_weight,
    down_weight,
    out_gain,
):
    return layer(
        a_lin,
        a_gate,
        conv_weight,
        ln_gain,
        ln_bias,
        proj_weight,
        residual,
        mix_gain,
        ffn_gain,
        out_gain,
        routes.T,
        route_weights.T,
        gate_weight,
        up_weight,
        down_weight,
    )


def solution(mesh):
    return jax.shard_map(
        per_device,
        mesh=mesh,
        in_specs=(
            P("sp", "tp"),
            P("sp", "tp"),
            P(None, "tp"),
            P("tp"),
            P("tp"),
            P(),
            P(("sp", "tp"), None),
            P(),
            P(),
            P(("sp", "tp"), None),
            P(("sp", "tp"), None),
            P("sp", None, "tp"),
            P("sp", None, "tp"),
            P("sp", "tp", None),
            P(),
        ),
        out_specs=P(("sp", "tp"), None),
        check_vma=False,
    )
```

```python
import jax
import jax.numpy as jnp
from jax import lax
from jax.experimental import pallas as pl
from jax.experimental.pallas import tpu as pltpu
from jax.sharding import PartitionSpec as P

D = 2048
D_A = 1024
HALF = D // 2
FFB = 896
CAP = 20
PAD = 24
TOK = 128
NG = 4
ROWS = 4 * CAP
PADROWS = 4 * PAD
EDGE = 32
EARLY = 16
MESH = pl.DeviceIdType.MESH
BF16 = jnp.bfloat16
F32 = jnp.float32

GROUPS = (
    ((0, 1), (0, 3), (1, 0), (3, 0)),
    ((1, 1), (3, 3), (3, 1), (1, 3)),
    ((2, 1), (2, 3), (1, 2), (3, 2)),
    ((0, 0), (0, 2), (2, 0), (2, 2)),
)
OFFS = tuple(o for g in GROUPS for o in g)
SELF = OFFS.index((0, 0))


def layer_kernel(
    lin_hbm,
    gate_hbm,
    conv_ref,
    lng_ref,
    lnb_ref,
    proj_hbm,
    resid_hbm,
    mixg_ref,
    ffng_ref,
    outg_ref,
    routes_ref,
    rweights_ref,
    wg_hbm,
    wu_hbm,
    wd_hbm,
    out_ref,
    lin,
    gatein,
    resid,
    proj,
    gsrc,
    small,
    taps,
    gbuf,
    padf,
    conv,
    act,
    branch,
    stream_ref,
    normed_ref,
    comb_ref,
    mixed,
    disp_ref,
    wgu,
    wd,
    outg,
    arecv,
    xbuf,
    hbuf,
    pbuf,
    precv,
    r1,
    r2,
    ret_s,
    ret_r,
    isem,
    wsem,
    c_s,
    c_r,
    a_s,
    a_r,
    g_s,
    g_r,
    s_s,
    s_r,
    t_s,
    t_r,
):
    sp = lax.axis_index("sp")
    tp = lax.axis_index("tp")
    z, x = lax.div(sp, 4), lax.rem(sp, 4)
    y, c = lax.div(tp, 2), lax.rem(tp, 2)

    def sp_at(dz, dx):
        return lax.rem(z + dz, 4) * 4 + lax.rem(x + dx, 4)

    up = lax.rem(y + 1, 4) * 2 + c
    down = lax.rem(y + 3, 4) * 2 + c
    mate = y * 2 + 1 - c

    icopies = [
        pltpu.make_async_copy(src, dst, isem.at[n])
        for n, (src, dst) in enumerate(
            ((lin_hbm, lin), (gate_hbm, gatein), (resid_hbm, resid), (proj_hbm, proj))
        )
    ]
    icopies[0].start()
    icopies[1].start()

    barrier = pltpu.get_barrier_semaphore()

    def greet(spi, tpi):
        pl.semaphore_signal(
            barrier, inc=1, device_id={"sp": spi, "tp": tpi}, device_id_type=MESH
        )

    for r in range(1, 8):
        greet(sp, lax.rem(tp + r, 8))
    for o in OFFS:
        if o != (0, 0):
            greet(sp_at(*o), tp)

    @pl.when(tp == 0)
    def _():
        for t in range(1, 8):
            greet(lax.rem(sp + 15, 16), t)

    def remote(src, dst, ssem, rsem, spi, tpi):
        return pltpu.make_async_remote_copy(
            src_ref=src,
            dst_ref=dst,
            send_sem=ssem,
            recv_sem=rsem,
            device_id={"sp": spi, "tp": tpi},
            device_id_type=MESH,
        )

    sends = []
    ccopies = {}

    def exchange(n, src, dst, spi, tpi):
        cp = remote(src, dst, c_s.at[n], c_r.at[n], spi, tpi)
        cp.start()
        ccopies[n] = cp
        sends.append(cp)

    def edge_of(t):
        return pl.ds(pl.multiple_of(lax.rem(t + 7, 8) * TOK + TOK - EDGE, EDGE), EDGE)

    def body_of(t):
        return pl.ds(pl.multiple_of(t * TOK, TOK), TOK)

    small[...] = jnp.zeros((40, TOK), BF16)
    small[0:31] = conv_ref[...]
    small[31:32] = lng_ref[...].reshape(1, TOK)
    small[32:33] = lnb_ref[...].reshape(1, TOK)
    taps[tp] = small[...]
    icopies[0].wait()
    icopies[1].wait()
    wcopies = []
    for j in range(7):
        cols = pl.ds(128 * j, 128)
        for h, w in enumerate((wg_hbm, wu_hbm)):
            wcopies.append(
                pltpu.make_async_copy(
                    w.at[0, :, cols], wgu.at[j, :, pl.ds(128 * h, 128)], wsem.at[2 * j + h]
                )
            )
    wcopies.append(pltpu.make_async_copy(wd_hbm.at[0], wd, wsem.at[14]))
    for cp in icopies[2:] + wcopies:
        cp.start()


    def gate(t):
        rows = pl.ds(TOK * t, TOK)
        g = gatein[rows, :].astype(F32)
        v = lin[rows, :].astype(F32) * (1.0 / (1.0 + jnp.exp(-g)))
        gsrc[rows, :] = v.astype(BF16)

    for r in range(8):
        gate(r)
    pl.semaphore_wait(barrier, 22 + jnp.minimum(tp, 1))
    peers = [(dy, o) for dy in range(4) for o in range(2)][1:]

    def peer(dy, o):
        return lax.rem(y + dy, 4) * 2 + (c if o == 0 else 1 - c)

    for n, p in enumerate(peers):
        t = peer(*p)
        exchange(14 + n, small, taps.at[tp], sp, t)
        exchange(n, gsrc.at[body_of(t)], gbuf.at[tp, pl.ds(EDGE, TOK)], sp, t)
        first = lax.div(8 - t, 8)
        exchange(
            7 + n, gsrc.at[edge_of(t)], gbuf.at[tp, pl.ds(0, EDGE)], lax.rem(sp + first, 16), t
        )
    own_edge = remote(
        gsrc.at[edge_of(0)],
        gbuf.at[tp, pl.ds(0, EDGE)],
        c_s.at[21],
        c_r.at[21],
        lax.rem(sp + 1, 16),
        tp,
    )

    @pl.when(tp == 0)
    def _():
        own_edge.start()

    @pl.when(tp > 0)
    def _():
        gbuf[tp, 0:EDGE] = gsrc[edge_of(tp), :]

    gbuf[tp, EDGE:] = gsrc[body_of(tp), :]

    lane = lax.broadcasted_iota(jnp.int32, (1, TOK), 1)
    code = lax.broadcasted_iota(jnp.int32, (16, TOK), 0)
    places, counts = [], jnp.zeros((16, TOK), F32)
    for k in range(2):
        e = routes_ref[k : k + 1, :]
        ez, ex = lax.shift_right_logical(e, 2), jnp.bitwise_and(e, 3)
        rel = jnp.bitwise_and(ez - z + 4, 3) * 4 + jnp.bitwise_and(ex - x + 4, 3)
        place = jnp.zeros_like(rel)
        for j, (dz, dx) in enumerate(OFFS):
            place = jnp.where(rel == dz * 4 + dx, j, place)
        places.append(place)
        counts = counts + jnp.where(code == place, 1.0, 0.0)
    earlier = lax.broadcasted_iota(jnp.int32, (TOK, TOK), 0) < lax.broadcasted_iota(
        jnp.int32, (TOK, TOK), 1
    )
    before = jnp.dot(
        counts.astype(BF16),
        jnp.where(earlier, 1.0, 0.0).astype(BF16),
        preferred_element_type=F32,
    )
    row = lax.broadcasted_iota(jnp.int32, (16 * PAD, TOK), 0)
    disp, comb = jnp.zeros((16 * PAD, TOK), F32), jnp.zeros((16 * PAD, TOK), F32)
    for k in range(2):
        slot = jnp.sum(jnp.where(code == places[k], before, 0.0), axis=0, keepdims=True)
        hit = row == places[k] * PAD + slot.astype(jnp.int32)
        disp = jnp.where(hit, 1.0, disp)
        comb = jnp.where(hit, rweights_ref[k : k + 1, :], comb)
    disp_ref[...] = disp.astype(BF16)
    comb = comb.T
    high = comb.astype(BF16)
    low = (comb - high.astype(F32)).astype(BF16)
    for i in range(NG):
        comb_ref[0, i] = high[:, PADROWS * i : PADROWS * (i + 1)]
        comb_ref[1, i] = low[:, PADROWS * i : PADROWS * (i + 1)]

    no_edge = jnp.logical_and(sp == 0, tp == 0)
    keep = jnp.where(no_edge, 0.0, 1.0)
    edge_mask = jnp.where(lax.broadcasted_iota(jnp.int32, (EDGE + TOK, TOK), 0) < EDGE, keep, 1.0)

    def filtered(b):
        padf[...] = gbuf[b].astype(F32) * edge_mask
        w = taps[b].astype(F32)
        total = w[0:1] * padf[2 : 2 + TOK, :]
        for k in range(1, 31):
            total = total + w[k : k + 1] * padf[2 + k : 2 + k + TOK, :]
        conv[b] = total
        return total, total * total

    def arrived(n):
        for k in (n, 7 + n, 14 + n):
            ccopies[k].wait_recv()
        dy, o = peers[n]
        return peer((4 - dy) % 4, o)

    sum1, sum2 = filtered(arrived(0))
    for n in range(1, 8):
        if n == 7:

            @pl.when(tp == 0)
            def _():
                own_edge.wait_recv()

        more1, more2 = filtered(tp) if n == 7 else filtered(arrived(n))
        sum1, sum2 = sum1 + more1, sum2 + more2
    mean = jnp.sum(sum1, axis=1, keepdims=True) / D_A
    var = jnp.sum(sum2, axis=1, keepdims=True) / D_A - mean * mean
    rstd = lax.rsqrt(var + 1e-05)

    @pl.loop(0, 8)
    def _(b):
        w = taps[b].astype(F32)
        v = (conv[b] - mean) * rstd * w[31:32] + w[32:33]
        act[:, pl.ds(pl.multiple_of(b * TOK, TOK), TOK)] = (v * (1.0 / (1.0 + jnp.exp(-v)))).astype(
            BF16
        )

    icopies[3].wait()

    @pl.loop(0, 2)
    def _(n):
        cols = pl.ds(pl.multiple_of(n * 1024, 1024), 1024)
        branch[:, cols] = jnp.dot(act[...], proj[:, cols], preferred_element_type=F32).astype(BF16)

    icopies[2].wait()
    mixg = mixg_ref[...].astype(F32).reshape(1, D)
    ffng = ffng_ref[...].astype(F32).reshape(1, D)

    @pl.loop(0, 4)
    def _(n):
        rows = pl.ds(pl.multiple_of(n * 32, 32), 32)
        b = branch[rows, :].astype(F32)
        scale = lax.rsqrt(jnp.mean(b * b, axis=1, keepdims=True) + 1e-06)
        st = resid[rows, :].astype(F32) + b * scale * mixg
        stream_ref[rows, :] = st
        scale = lax.rsqrt(jnp.mean(st * st, axis=1, keepdims=True) + 1e-06)
        normed_ref[rows, :] = (st * scale * ffng).astype(BF16)

    ag = [dict() for _ in range(NG)]

    def ag_copy(i, n, src, dst, tpi):
        cp = remote(src, dst, g_s.at[i, n], g_r.at[i, n], sp, tpi)
        cp.start()
        ag[i][n] = cp
        sends.append(cp)

    acopies = {}

    def dispatch(i):
        for j in range(4 * i, 4 * i + 4):
            if j != SELF:
                acopies[j] = remote(
                    outg.at[j], arecv.at[j], a_s.at[j], a_r.at[j], sp_at(*OFFS[j]), tp
                )
                acopies[j].start()
                sends.append(acopies[j])

    for i in range(NG):
        rows = jnp.dot(
            disp_ref[PADROWS * i : PADROWS * (i + 1), :],
            normed_ref[...],
            preferred_element_type=F32,
        )
        outg[4 * i : 4 * i + 4] = rows.astype(BF16).reshape(4, PAD, D)
        if i == SELF // 4:
            xbuf[i, 0, 0, 0:EARLY] = outg[SELF, 0:EARLY]
            early = pl.ds(0, EARLY)
            ag_copy(i, 8, xbuf.at[i, 0, 0, early], xbuf.at[i, 0, 3, early], up)
            ag_copy(i, 9, xbuf.at[i, 0, 0, early], xbuf.at[i, 0, 1, early], down)
        if i == 0:
            dispatch(0)

    r_i = lax.broadcasted_iota(jnp.int32, (ROWS, PADROWS), 0)
    c_i = lax.broadcasted_iota(jnp.int32, (ROWS, PADROWS), 1)
    q_i = sum((r_i >= CAP * k).astype(jnp.int32) for k in (1, 2, 3))
    compact = (c_i == r_i + (PAD - CAP) * q_i).astype(F32).astype(BF16)
    r_e = lax.broadcasted_iota(jnp.int32, (PADROWS, ROWS), 0)
    c_e = lax.broadcasted_iota(jnp.int32, (PADROWS, ROWS), 1)
    q_e = sum((c_e >= CAP * k).astype(jnp.int32) for k in (1, 2, 3))
    expand = (r_e == c_e + (PAD - CAP) * q_e).astype(F32).astype(BF16)

    def gather1(i):
        blocks = []
        for j in range(4 * i, 4 * i + 4):
            if j == SELF:
                blocks.append(outg[j])
            else:
                acopies[j].wait_recv()
                blocks.append(arecv[j])
        own = jnp.dot(compact, jnp.concatenate(blocks, axis=0), preferred_element_type=F32)
        start = EARLY if i == SELF // 4 else 0
        rest = pl.ds(start, ROWS - start)
        xbuf[i, 0, 0, start:] = own.astype(BF16)[start:]
        src = xbuf.at[i, 0, 0, rest]
        ag_copy(i, 0, src, xbuf.at[i, 0, 3, rest], up)
        ag_copy(i, 1, src, xbuf.at[i, 0, 1, rest], down)
        ag_copy(i, 2, xbuf.at[i, 0, 0], xbuf.at[i, 1, 0], mate)

    lo, hi = pl.ds(0, HALF), pl.ds(HALF, HALF)

    def gather2(i):
        ag[i][0].wait_recv()
        if i == SELF // 4:
            ag[i][8].wait_recv()
        ag_copy(i, 3, xbuf.at[i, 0, 3, :, lo], xbuf.at[i, 0, 2, :, lo], up)
        ag_copy(i, 6, xbuf.at[i, 0, 3], xbuf.at[i, 1, 3], mate)
        ag[i][1].wait_recv()
        if i == SELF // 4:
            ag[i][9].wait_recv()
        ag_copy(i, 4, xbuf.at[i, 0, 1, :, hi], xbuf.at[i, 0, 2, :, hi], down)
        ag_copy(i, 5, xbuf.at[i, 0, 1], xbuf.at[i, 1, 1], mate)

    def relay(i):
        ag[i][3].wait_recv()
        ag[i][4].wait_recv()
        ag_copy(i, 7, xbuf.at[i, 0, 2], xbuf.at[i, 1, 2], mate)

    def ready(i):
        for n in (2, 5, 6, 7):
            ag[i][n].wait_recv()

    rs = [dict() for _ in range(NG)]

    def rs_copy(i, n, src, dst, tpi):
        cp = remote(src, dst, s_s.at[i, n], s_r.at[i, n], sp, tpi)
        cp.start()
        rs[i][n] = cp
        sends.append(cp)

    def hidden(i):
        if i == 0:
            for cp in wcopies[:14]:
                cp.wait()

        @pl.loop(0, 7)
        def _(j):
            gu = jnp.dot(xbuf[i].reshape(8 * ROWS, D), wgu[j], preferred_element_type=F32)
            g, u = gu[:, :128], gu[:, 128:]
            h = g * (1.0 / (1.0 + jnp.exp(-g))) * u
            hbuf[:, pl.ds(pl.multiple_of(j * 128, 128), 128)] = h.astype(BF16)

    def partial(i):
        if i == 0:
            wcopies[14].wait()
        for half in (1, 0):
            for cols in (lo, hi):
                p = jnp.dot(
                    hbuf[4 * ROWS * half : 4 * ROWS * (half + 1), :],
                    wd[:, cols],
                    preferred_element_type=F32,
                )
                pbuf[i, half, :, :, cols] = p.astype(BF16).reshape(4, ROWS, HALF)
                if half == 1:
                    n = 0 if cols is lo else 7
                    rs_copy(i, n, pbuf.at[i, 1, :, :, cols], precv.at[i, :, :, cols], mate)

    def both(i, k, cols):
        return pbuf[i, 0, k, :, cols].astype(F32) + precv[i, k, :, cols].astype(F32)

    def scatter1(i):
        rs[i][0].wait_recv()
        pbuf[i, 0, 2, :, :HALF] = both(i, 2, slice(0, HALF)).astype(BF16)
        rs_copy(i, 1, pbuf.at[i, 0, 2, :, lo], r1.at[i, 0], up)
        rs[i][7].wait_recv()
        pbuf[i, 0, 2, :, HALF:] = both(i, 2, slice(HALF, D)).astype(BF16)
        rs_copy(i, 2, pbuf.at[i, 0, 2, :, hi], r1.at[i, 1], down)
        pbuf[i, 0, 1, :, HALF:] = both(i, 1, slice(HALF, D)).astype(BF16)
        rs_copy(i, 3, pbuf.at[i, 0, 1, :, hi], r2.at[i, 0, :, hi], up)
        pbuf[i, 0, 3, :, :HALF] = both(i, 3, slice(0, HALF)).astype(BF16)
        rs_copy(i, 4, pbuf.at[i, 0, 3, :, lo], r2.at[i, 1, :, lo], down)

    def scatter2(i):
        rs[i][1].wait_recv()
        pbuf[i, 0, 1, :, :HALF] = (both(i, 1, slice(0, HALF)) + r1[i, 0].astype(F32)).astype(BF16)
        rs_copy(i, 5, pbuf.at[i, 0, 1, :, lo], r2.at[i, 0, :, lo], up)
        rs[i][2].wait_recv()
        pbuf[i, 0, 3, :, HALF:] = (both(i, 3, slice(HALF, D)) + r1[i, 1].astype(F32)).astype(BF16)
        rs_copy(i, 6, pbuf.at[i, 0, 3, :, hi], r2.at[i, 1, :, hi], down)

    tcopies = {}

    def give_back(i):
        for n in (3, 4, 5, 6):
            rs[i][n].wait_recv()
        total = both(i, 0, slice(None)) + r2[i, 0].astype(F32) + r2[i, 1].astype(F32)
        padded = jnp.dot(expand, total.astype(BF16), preferred_element_type=F32)
        padded = padded.astype(BF16).reshape(4, PAD, D)
        for q in range(4):
            j = 4 * i + q
            dz, dx = OFFS[j]
            if j == SELF:
                ret_r[j] = padded[q]
            else:
                ret_s[j] = padded[q]
                tcopies[j] = remote(
                    ret_s.at[j], ret_r.at[j], t_s.at[j], t_r.at[j], sp_at(4 - dz, 4 - dx), tp
                )
                tcopies[j].start()
                sends.append(tcopies[j])

    gather1(0)
    dispatch(1)
    gather1(1)
    dispatch(2)
    gather2(0)
    gather1(2)
    dispatch(3)
    gather2(1)
    relay(0)
    ready(0)
    hidden(0)
    gather1(3)
    gather2(2)
    relay(1)
    partial(0)
    ready(1)
    scatter1(0)
    hidden(1)
    gather2(3)
    scatter2(0)
    relay(2)
    partial(1)
    ready(2)
    scatter1(1)
    hidden(2)
    scatter2(1)
    relay(3)
    give_back(0)
    partial(2)
    ready(3)
    scatter1(2)
    hidden(3)
    scatter2(2)
    give_back(1)
    partial(3)
    scatter1(3)
    give_back(2)
    scatter2(3)
    give_back(3)
    for i in range(NG):
        if i == NG - 1:
            mixed[...] = mix
        for j in range(4 * i, 4 * i + 4):
            if j != SELF:
                tcopies[j].wait_recv()
        ret = ret_r[4 * i : 4 * i + 4].reshape(PADROWS, D)
        part = jnp.dot(comb_ref[0, i], ret, preferred_element_type=F32)
        part = part + jnp.dot(comb_ref[1, i], ret, preferred_element_type=F32)
        mix = part if i == 0 else mix + part if i < NG - 1 else mixed[...] + part
    scale = lax.rsqrt(jnp.mean(mix * mix, axis=1, keepdims=True) + 1e-06)
    result = stream_ref[...] + mix * scale * outg_ref[...].astype(F32).reshape(1, D)
    out_ref[...] = result.astype(BF16)
    for cp in sends:
        cp.wait_send()

    @pl.when(tp == 0)
    def _():
        own_edge.wait_send()


def layer(*operands):
    vmem = pl.BlockSpec(memory_space=pltpu.VMEM)
    hbm = pl.BlockSpec(memory_space=pl.ANY)
    dma = pltpu.SemaphoreType.DMA
    return pl.pallas_call(
        layer_kernel,
        out_shape=jax.ShapeDtypeStruct((TOK, D), BF16),
        in_specs=[hbm, hbm, vmem, vmem, vmem, hbm, hbm, vmem, vmem, vmem, vmem, vmem, hbm, hbm, hbm],
        out_specs=vmem,
        scratch_shapes=[
            pltpu.VMEM((8 * TOK, TOK), BF16),
            pltpu.VMEM((8 * TOK, TOK), BF16),
            pltpu.VMEM((TOK, D), BF16),
            pltpu.VMEM((D_A, D), BF16),
            pltpu.VMEM((8 * TOK, TOK), BF16),
            pltpu.VMEM((40, TOK), BF16),
            pltpu.VMEM((8, 40, TOK), BF16),
            pltpu.VMEM((8, EDGE + TOK, TOK), BF16),
            pltpu.VMEM((EDGE + TOK, TOK), F32),
            pltpu.VMEM((8, TOK, TOK), F32),
            pltpu.VMEM((TOK, D_A), BF16),
            pltpu.VMEM((TOK, D), BF16),
            pltpu.VMEM((TOK, D), F32),
            pltpu.VMEM((TOK, D), BF16),
            pltpu.VMEM((2, NG, TOK, PADROWS), BF16),
            pltpu.VMEM((TOK, D), F32),
            pltpu.VMEM((16 * PAD, TOK), BF16),
            pltpu.VMEM((7, D, 256), BF16),
            pltpu.VMEM((FFB, D), BF16),
            pltpu.VMEM((16, PAD, D), BF16),
            pltpu.VMEM((16, PAD, D), BF16),
            pltpu.VMEM((NG, 2, 4, ROWS, D), BF16),
            pltpu.VMEM((8 * ROWS, FFB), BF16),
            pltpu.VMEM((NG, 2, 4, ROWS, D), BF16),
            pltpu.VMEM((NG, 4, ROWS, D), BF16),
            pltpu.VMEM((NG, 2, ROWS, HALF), BF16),
            pltpu.VMEM((NG, 2, ROWS, D), BF16),
            pltpu.VMEM((16, PAD, D), BF16),
            pltpu.VMEM((16, PAD, D), BF16),
            dma((4,)),
            dma((15,)),
            dma((22,)),
            dma((22,)),
            dma((16,)),
            dma((16,)),
            dma((NG, 10)),
            dma((NG, 10)),
            dma((NG, 8)),
            dma((NG, 8)),
            dma((16,)),
            dma((16,)),
        ],
        compiler_params=pltpu.CompilerParams(
            collective_id=0, has_side_effects=True, vmem_limit_bytes=62 * 1024 * 1024
        ),
        name="layer",
    )(*operands)


def per_device(
    a_lin,
    a_gate,
    conv_weight,
    ln_gain,
    ln_bias,
    proj_weight,
    residual,
    mix_gain,
    ffn_gain,
    routes,
    route_weights,
    gate_weight,
    up_weight,
    down_weight,
    out_gain,
):
    return layer(
        a_lin,
        a_gate,
        conv_weight,
        ln_gain,
        ln_bias,
        proj_weight,
        residual,
        mix_gain,
        ffn_gain,
        out_gain,
        routes.T,
        route_weights.T,
        gate_weight,
        up_weight,
        down_weight,
    )


def solution(mesh):
    return jax.shard_map(
        per_device,
        mesh=mesh,
        in_specs=(
            P("sp", "tp"),
            P("sp", "tp"),
            P(None, "tp"),
            P("tp"),
            P("tp"),
            P(),
            P(("sp", "tp"), None),
            P(),
            P(),
            P(("sp", "tp"), None),
            P(("sp", "tp"), None),
            P("sp", None, "tp"),
            P("sp", None, "tp"),
            P("sp", "tp", None),
            P(),
        ),
        out_specs=P(("sp", "tp"), None),
        check_vma=False,
    )
```
